256 devices in a mesh: gr: 2 (over z_hi), sp: 16 (over z_lo, y), tp: 8 (over x, core).
Axes of the slice: x: 4, y: 4, z: 8 (z_hi: 2, z_lo: 4; z = z_hi * 4 + z_lo), core: 2. Of those that a mesh axis runs over, the one named last changes fastest.
Arguments:
- prompt: bfloat16 [256, 256, 1024], P('gr', 'sp'), parts along dimension 0, may hold values from -6 to 6
- w_key: bfloat16 [1024, 8, 128], P(None, 'tp'), may hold values from -0.1875 to 0.1875
- w_value: bfloat16 [1024, 8, 128], P(None, 'tp'), may hold values from -0.1875 to 0.1875
- w_in_gate: bfloat16 [2, 1024, 8], P(None, None, 'tp'), may hold values from -0.1875 to 0.1875
- w_forget_gate: bfloat16 [2, 1024, 8], P(None, None, 'tp'), may hold values from -0.1875 to 0.1875
- in_bias: float32 [2, 8], P(None, 'tp'), may hold values from -6 to 0, as said below
- forget_bias: float32 [2, 8], P(None, 'tp'), may hold values from 1 to 10, as said below
- query: bfloat16 [256, 8, 128], P(('gr', 'sp'), 'tp'), parts along dimension 0, may hold values from -6 to 6
- w_out: bfloat16 [8, 128, 1024], P('tp'), may hold values from -0.5 to 0.5
Outputs:
- memory: bfloat16 [2, 256, 8, 128, 128], P(None, ('gr', 'sp'), 'tp'), parts along dimension 1
- normalizer: float32 [2, 256, 8, 128], P(None, ('gr', 'sp'), 'tp'), parts along dimension 1
- stabilizer: float32 [2, 256, 8], P(None, ('gr', 'sp'), 'tp'), parts along dimension 1
- read: bfloat16 [256, 1024], P(('gr', 'sp'), 'tp'), parts along dimension 0
The draws below stay inside these ranges and needn't reach their ends.
There are 2 independent parts, one for each index of `gr`. The reference program is written for one: setup_inputs(seed, part) draws one part's arguments, and reference() takes and returns one part's arrays. A program takes and returns all parts, laid end to end along the dimension named above; an argument that names none is the same for every part. Nothing has to cross between parts.
Inputs may be any that keep to these rules, and one draw needn't show every extreme that they name: forget_bias lies between 1 and 10; the per-head share of memory kept over the whole prompt is spread between a few and some ninety percent. in_bias lies between -6 and 0.
All inputs are finite; a program needn't handle non-finite values.
Results may differ from the reference program's by a relative error of at most 0.015.
Values may be sent and summed in bfloat16 or wider, within the bound.
A program may use at most 64 MiB of HBM per device.

```python
import math
import jax
import jax.numpy as jnp
from jax import lax

D = 1024
HEADS = 8
HEAD_DIM = 128
SEQS = 128
SEQ_LEN = 256


def draw_forget_bias(key, part):
    kept_share = jnp.exp(jax.random.uniform(key, (2, HEADS), jnp.float32, math.log(0.05), math.log(0.9)))
    chain_loss = -jnp.log(kept_share) / 1.65
    return -jnp.log(jnp.expm1(chain_loss / SEQ_LEN))


def draw_in_bias(key, part):
    centre = -0.5 * math.log(SEQ_LEN) - 1.0
    offset = jax.random.uniform(key, (2, HEADS), jnp.float32, -1.0, 1.0)
    return offset + centre


def block_scale(stream_key, dims, shards, smallest, high):
    loudness, own = 1.0, jax.random.fold_in(stream_key, 6)
    for position, shards_of in shards:
        steps = jnp.exp(jax.random.uniform(jax.random.fold_in(own, position), (shards_of,), jnp.float32, smallest / len(shards), high / len(shards)))
        loudness = loudness * jnp.repeat(steps, dims[position] // shards_of).reshape([-1 if axis == position else 1 for axis in range(len(dims))])
    return loudness


def gaussian(key, extent, scale, reach, pieces=(), kind=jnp.bfloat16):
    loudness = block_scale(key, extent, pieces, -0.22, 0.18) if pieces else 1.0
    array = jax.random.normal(key, extent, jnp.float32) * scale * loudness
    return jnp.minimum(jnp.maximum(array, -reach), reach).astype(kind)


def setup_inputs(seed: int = 0, part: int = 0) -> dict:
    keys = jax.random.split(jax.random.key(seed), 10)
    part_keys = jax.random.split(jax.random.fold_in(keys[9], part), 10)
    prompt = gaussian(part_keys[0], (SEQS, SEQ_LEN, D), 1.0, 6.0, ((1, 16),))
    w_key = gaussian(keys[1], (D, HEADS, HEAD_DIM), D ** -0.5, 0.1875, ((1, 8),))
    w_value = gaussian(keys[2], (D, HEADS, HEAD_DIM), D ** -0.5, 0.1875, ((1, 8),))
    w_in_gate = gaussian(keys[3], (2, D, HEADS), D ** -0.5, 0.1875, ((2, 8),))
    w_forget_gate = gaussian(keys[4], (2, D, HEADS), D ** -0.5, 0.1875, ((2, 8),))
    in_bias = draw_in_bias(jax.random.fold_in(keys[9], 71), part)
    forget_bias = draw_forget_bias(jax.random.fold_in(keys[9], 71), part)
    query = gaussian(part_keys[7], (SEQS, HEADS, HEAD_DIM), 1.0, 6.0, ((0, 16), (1, 8)))
    w_out = gaussian(keys[8], (HEADS, HEAD_DIM, D), (HEADS * HEAD_DIM // 9) ** -0.5, 0.5, ((0, 8),))
    return dict(prompt=prompt, w_key=w_key, w_value=w_value, w_in_gate=w_in_gate, w_forget_gate=w_forget_gate, in_bias=in_bias, forget_bias=forget_bias, query=query, w_out=w_out)


highest = lax.Precision.HIGHEST


def summary(scaled, float_values, in_log, forget_log, backward):
    total_forget = jnp.sum(forget_log, axis=1)
    running = jnp.cumsum(forget_log, axis=1)
    if backward:
        log_weight = in_log + running - forget_log
    else:
        log_weight = in_log + total_forget[:, None, :] - running
    stable = jnp.maximum(total_forget, jnp.max(log_weight, axis=1))
    weight = jnp.exp(log_weight - stable[:, None, :])
    weighted = scaled * weight[..., None]
    memory = jnp.einsum('bshd,bshe->bhde', weighted, float_values, precision=highest)
    normal = jnp.sum(weighted, axis=1)
    return memory, normal, stable


def read_out(memory_bf, normal, stable, query_f):
    cells = memory_bf.astype(jnp.float32)
    numerator = jnp.sum(query_f[..., :, None] * cells, axis=-2)
    denominator = jnp.sum(query_f * normal, axis=-1)
    floor_value = jnp.maximum(jnp.maximum(jnp.abs(denominator), jnp.exp(-stable)), 1.0)
    return numerator / floor_value[..., None]


def reference(prompt, w_key, w_value, w_in_gate, w_forget_gate, in_bias, forget_bias, query, w_out):
    token_rows = prompt.astype(jnp.float32)
    key_rows = jnp.einsum('bsd,dhe->bshe', token_rows, w_key.astype(jnp.float32), precision=highest).astype(jnp.bfloat16)
    value_rows = jnp.einsum('bsd,dhe->bshe', token_rows, w_value.astype(jnp.float32), precision=highest).astype(jnp.bfloat16)
    in_pre = jnp.einsum('bsd,gdh->bsgh', token_rows, w_in_gate.astype(jnp.float32), precision=highest) + in_bias
    forget_pre = jnp.einsum('bsd,gdh->bsgh', token_rows, w_forget_gate.astype(jnp.float32), precision=highest) + forget_bias
    scaled = key_rows.astype(jnp.float32) * (key_rows.shape[-1] ** -0.5)
    float_values = value_rows.astype(jnp.float32)
    query_f = query.astype(jnp.float32)
    memories = []
    normals = []
    stables = []
    reads = []
    for course in range(2):
        memory, normal, stable = summary(scaled, float_values, in_pre[:, :, course, :],
                                         jax.nn.log_sigmoid(forget_pre[:, :, course, :]), course == 1)
        memory_bf = memory.astype(jnp.bfloat16)
        memories.append(memory_bf)
        normals.append(normal)
        stables.append(stable)
        reads.append(read_out(memory_bf, normal, stable, query_f))
    hidden = (reads[0] + reads[1]).astype(jnp.bfloat16)
    read = jnp.einsum('bhd,hde->be', hidden.astype(jnp.float32), w_out.astype(jnp.float32), precision=highest).astype(jnp.bfloat16)
    return (jnp.stack(memories), jnp.stack(normals), jnp.stack(stables), read)
```

```python
import functools

import jax
import jax.numpy as jnp
from jax import lax
from jax.experimental import pallas as pl
from jax.experimental.pallas import tpu as pltpu
from jax.sharding import PartitionSpec as P

MESH = pl.DeviceIdType.MESH
F32 = jnp.float32
BF16 = jnp.bfloat16
HIGHEST = lax.Precision.HIGHEST


def nt(a, b):
    return lax.dot_general(a, b, (((1,), (1,)), ((), ())), preferred_element_type=F32)


def tn(a, b):
    return lax.dot_general(a, b, (((0,), (0,)), ((), ())), preferred_element_type=F32)


def iota(shape, axis):
    return lax.broadcasted_iota(jnp.int32, shape, axis)


def kernel(
    n, tpn,
    prompt, wk_hbm, wv_hbm, wo_hbm, ig_hbm, fg_hbm, ib_hbm, fb_hbm, q_hbm,
    membuf, norm_out, stab_out, read_out,
    xall, wkv, wo, in_gate, forget_gate, in_bias, forget_bias, query,
    wg, kvs, kvn, kvf, gsend, grecv, xfar, wb, qb, acc, num, nrm, parts, got,
    wsem, lsem, fsend, frecv, nsend, nrecv, gsem, grsem, xsend, xrecv, dsend, drecv, psend, precv,
):
    sp = lax.axis_index("sp")
    tp = lax.axis_index("tp")
    half = n // 2
    cores = 2
    chips = tpn // cores
    seqs, sources, block, depth = xfar.shape
    rows = seqs * block
    width = wo.shape[0]
    side = sp // half
    local = sp - side * half
    near_base = side * half
    far_base = half - near_base
    x, c = tp // cores, lax.rem(tp, cores)
    partner = x * cores + 1 - c

    barrier = pltpu.get_barrier_semaphore()
    for k in range(1, n):
        pl.semaphore_signal(
            barrier, inc=1, device_id={"sp": lax.rem(sp + k, n)}, device_id_type=MESH
        )
    for j in range(1, tpn):
        pl.semaphore_signal(
            barrier, inc=1, device_id={"tp": lax.rem(tp + j, tpn)}, device_id_type=MESH
        )

    weights = [
        pltpu.make_async_copy(wk_hbm, wkv.at[:, :width], wsem.at[0]),
        pltpu.make_async_copy(wv_hbm, wkv.at[:, width:], wsem.at[1]),
        pltpu.make_async_copy(ig_hbm, in_gate, wsem.at[2]),
        pltpu.make_async_copy(fg_hbm, forget_gate, wsem.at[3]),
        pltpu.make_async_copy(ib_hbm, in_bias, wsem.at[4]),
        pltpu.make_async_copy(fb_hbm, forget_bias, wsem.at[5]),
        pltpu.make_async_copy(q_hbm, query, wsem.at[6]),
        pltpu.make_async_copy(wo_hbm, wo, wsem.at[7]),
    ]

    def near_of(k):
        return near_base + lax.rem(local + k, half)

    def far_of(k):
        return far_base + lax.rem(local + k, half)

    def far_from(k):
        return lax.rem(local + half - k, half)

    def load(k):
        return pltpu.make_async_copy(
            prompt.at[pl.ds(near_of(k) * seqs, seqs)],
            xall.at[pl.ds(near_of(k) * seqs, seqs)],
            lsem.at[k],
        )

    def load_far():
        part = pl.ds(far_base * seqs, half * seqs)
        return pltpu.make_async_copy(prompt.at[part], xall.at[part], lsem.at[half])

    def send_far(k):
        dest = far_of(k)
        return pltpu.make_async_remote_copy(
            src_ref=prompt.at[dest * seqs + tp],
            dst_ref=xfar.at[tp, local],
            send_sem=fsend.at[k],
            recv_sem=frecv.at[k],
            device_id={"sp": dest},
            device_id_type=MESH,
        )

    def send_near(k):
        return pltpu.make_async_remote_copy(
            src_ref=kvs.at[k],
            dst_ref=kvn.at[local],
            send_sem=nsend.at[k],
            recv_sem=nrecv.at[k],
            device_id={"sp": near_of(k)},
            device_id_type=MESH,
        )

    def send_gates(k):
        dest = lax.rem(sp + k, n)
        return pltpu.make_async_remote_copy(
            src_ref=gsend.at[dest],
            dst_ref=grecv.at[sp],
            send_sem=gsem.at[k],
            recv_sem=grsem.at[k],
            device_id={"sp": dest},
            device_id_type=MESH,
        )

    def spread(j, k):
        piece = xfar.at[tp, far_from(k)]
        return pltpu.make_async_remote_copy(
            src_ref=piece,
            dst_ref=piece,
            send_sem=xsend.at[j, k],
            recv_sem=xrecv.at[j, k],
            device_id={"tp": lax.rem(x + j, chips) * cores + c},
            device_id_type=MESH,
        )

    def hand(j, k):
        origin = lax.rem(x + chips - j, chips) * cores + c
        piece = xfar.at[origin, far_from(k)]
        return pltpu.make_async_remote_copy(
            src_ref=piece,
            dst_ref=piece,
            send_sem=dsend.at[j, k],
            recv_sem=drecv.at[j, k],
            device_id={"tp": partner},
            device_id_type=MESH,
        )

    def give(j):
        peer = lax.rem(tp + j, tpn)
        return pltpu.make_async_remote_copy(
            src_ref=parts.at[peer],
            dst_ref=got.at[j],
            send_sem=psend.at[j],
            recv_sem=precv.at[j],
            device_id={"tp": peer},
            device_id_type=MESH,
        )

    for copy in weights[:4]:
        copy.start()
    for k in list(range(1, half)) + [0]:
        load(k).start()
    load_far().start()
    for copy in weights[4:]:
        copy.start()
    pl.semaphore_wait(barrier, n - 1 + tpn - 1)
    for k in range(half):
        send_far(k).start()

    for copy in weights[:4]:
        copy.wait()
    wg[...] = jnp.concatenate(
        [in_gate[...].astype(F32), forget_gate[...].astype(F32), jnp.zeros((wg.shape[0] - 4, depth), F32)],
        axis=0,
    ).astype(BF16)

    def rows_of(dest):
        return xall[pl.ds(dest * seqs, seqs)].reshape(rows, depth)

    def gates_to(dest):
        gsend[pl.ds(dest, 1)] = nt(wg[...], rows_of(dest))[: gsend.shape[1]][None]

    for k in list(range(1, half)) + [0]:
        load(k).wait()
        dest = near_of(k)
        both = jnp.dot(rows_of(dest), wkv[...], preferred_element_type=F32).astype(BF16)
        gates_to(dest)
        if k:
            kvs[k] = both
            send_near(k).start()
        else:
            kvn[pl.ds(local, 1)] = both[None]
    load_far().wait()
    for k in range(half):
        gates_to(far_of(k))
    grecv[pl.ds(sp, 1)] = gsend[pl.ds(sp, 1)]
    for k in range(1, n):
        send_gates(k).start()

    for copy in weights[4:]:
        copy.wait()
    turned = query[...].astype(F32).T
    for q in range(seqs):
        qb[q] = jnp.broadcast_to(turned[:, q : q + 1], (width, width))

    def weigh():
        for k in range(1, n):
            send_gates(k).wait_recv()
        lane = iota((rows, rows), 1)
        line = iota((rows, rows), 0)
        same = (lane // block) == (line // block)
        upto = (same & (line <= lane)).astype(F32)
        whole = same.astype(F32)
        before = (
            (iota((2 * n, 2 * n), 0) // n == iota((2 * n, 2 * n), 1) // n)
            & (iota((2 * n, 2 * n), 1) < iota((2 * n, 2 * n), 0))
        ).astype(F32)
        pre = [
            grecv[:, i, :] + (in_bias if i < 2 else forget_bias)[0:1, i % 2 : i % 2 + 1]
            for i in range(4)
        ]
        forget_pre = jnp.concatenate(pre[2:], axis=0)
        forget = jnp.minimum(forget_pre, 0.0) - jnp.log1p(jnp.exp(-jnp.abs(forget_pre)))
        inside = jnp.dot(forget, upto, preferred_element_type=F32, precision=HIGHEST)
        sums = jnp.dot(forget, whole, preferred_element_type=F32, precision=HIGHEST)
        running = jnp.dot(before, sums, preferred_element_type=F32, precision=HIGHEST) + inside
        totals = [jnp.sum(sums[g * n : (g + 1) * n], axis=0, keepdims=True) for g in range(2)]
        logs = [
            pre[0] + totals[0] - running[:n],
            pre[1] + running[n:] - forget[n:],
        ]
        peak = jnp.concatenate(
            [jnp.maximum(totals[g], jnp.max(logs[g], axis=0, keepdims=True)) for g in range(2)]
            + [jnp.zeros((6, rows), F32)],
            axis=0,
        )
        spot = iota(peak.shape, 1)
        step = 1
        while step < block:
            low, high = pltpu.roll(peak, step, 1), pltpu.roll(peak, rows - step, 1)
            peak = jnp.maximum(peak, jnp.where((spot & step) != 0, low, high))
            step *= 2
        weight = [jnp.exp(logs[g] - peak[g : g + 1]) * width ** (-0.5) for g in range(2)]
        first = side == 0
        parted = [jnp.where(first, w[:half], w[half:]) for w in weight]
        parted += [jnp.where(first, w[half:], w[:half]) for w in weight]
        columns = jnp.concatenate(parted, axis=0).T
        for i in range(4):
            for q in range(seqs):
                for s in range(half):
                    j = i * half + s
                    wb[i, q, s] = jnp.broadcast_to(
                        columns[q * block : (q + 1) * block, j : j + 1], (block, width)
                    )
        own = iota((seqs, rows), 1) // block == iota((seqs, rows), 0)
        return [
            jnp.max(jnp.where(own, peak[g : g + 1], -jnp.inf), axis=1, keepdims=True)
            for g in range(2)
        ]

    def outer(kv, i, q):
        lines = slice(q * block, (q + 1) * block)
        keys = kv[:, lines, :width].reshape(half * block, width)
        values = kv[:, lines, width:].reshape(half * block, width).astype(F32)
        w0 = wb[2 * i, q].reshape(half * block, width)
        w1 = wb[2 * i + 1, q].reshape(half * block, width)
        weighted = jnp.concatenate([values * w0, values * w1], axis=1).astype(BF16)
        keys_f = keys.astype(F32)
        sums = [jnp.sum(keys_f * w, axis=0, keepdims=True) for w in (w0, w1)]
        return tn(keys, weighted), sums

    def project(k):
        source = far_from(k)
        lines = xfar[:, pl.ds(source, 1)].reshape(rows, depth)
        kvf[pl.ds(source, 1)] = jnp.dot(
            lines, wkv[...], preferred_element_type=F32
        ).astype(BF16)[None]

    lag_hand, lag_project = 2, 4
    stable = None
    for step in range(half + lag_project):
        if step < half:
            send_far(step).wait_recv()
            for j in (1, 3, 2):
                spread(j, step).start()
            hand(0, step).start()
        k = step - lag_hand
        if 0 <= k < half:
            for j in (1, 3, 2):
                spread(j, k).wait_recv()
                hand(j, k).start()
        if step == half - 1:
            stable = weigh()
        if step == half:
            for k in range(1, half):
                send_near(k).wait_recv()
            for q in range(seqs):
                acc[q], sums = outer(kvn, 0, q)
                for g in range(2):
                    nrm[g, q : q + 1] = sums[g]
        k = step - lag_project
        if 0 <= k < half:
            for j in range(chips):
                hand(j, k).wait_recv()
            project(k)

    for q in range(seqs):
        more, sums = outer(kvf, 1, q)
        memory = (acc[q] + more).astype(BF16)
        back = memory.astype(F32)
        for g in range(2):
            membuf[g, q, 0] = memory[:, g * width : (g + 1) * width]
            num[g, q : q + 1] = jnp.sum(
                qb[q] * back[:, g * width : (g + 1) * width], axis=0, keepdims=True
            )
            total = nrm[g, q : q + 1] + sums[g]
            nrm[g, q : q + 1] = total
            norm_out[g, q] = total

    hidden = jnp.zeros((seqs, width), F32)
    queries = query[...].astype(F32)
    for g in range(2):
        under = jnp.abs(jnp.sum(queries * nrm[g], axis=1, keepdims=True))
        floor = jnp.maximum(jnp.exp(-stable[g]), 1.0)
        hidden = hidden + num[g] / jnp.maximum(under, floor)
        square = iota((seqs, width), 1) == iota((seqs, width), 0)
        row = jnp.sum(jnp.where(square, stable[g], 0.0), axis=0, keepdims=True)
        stab_out[g] = row[:, :seqs]
    terms = jnp.dot(hidden.astype(BF16), wo[...], preferred_element_type=F32)
    share = terms.shape[1] // tpn
    for t in range(tpn):
        parts[t] = terms[:, t * share : (t + 1) * share]
    for j in range(1, tpn):
        give(j).start()
    for k in range(half):
        send_far(k).wait_send()
        for j in range(1, chips):
            spread(j, k).wait_send()
        for j in range(chips):
            hand(j, k).wait_send()
    for k in range(1, half):
        send_near(k).wait_send()
    for k in range(1, n):
        send_gates(k).wait_send()
    total = parts[tp]
    for j in range(1, tpn):
        give(j).wait()
        total = total + got[j]
    read_out[...] = total.astype(BF16)


def publish(count, *refs):
    sources, targets, sems = refs[:count], refs[count : 2 * count], refs[2 * count]
    copies = [
        pltpu.make_async_copy(a, b, sems.at[i]) for i, (a, b) in enumerate(zip(sources, targets))
    ]
    for copy in copies:
        copy.start()
    for copy in copies:
        copy.wait()


def solution(mesh):
    n, tpn = mesh.shape["sp"], mesh.shape["tp"]

    def body(prompt, w_key, w_value, w_in_gate, w_forget_gate, in_bias, forget_bias, query, w_out):
        depth, heads, width = w_key.shape
        seqs = prompt.shape[0] // n
        block = prompt.shape[1]
        rows = seqs * block
        half = n // 2
        chips = tpn // 2
        wo = w_out.reshape(heads * width, -1)
        columns = wo.shape[1]
        any_ = pl.BlockSpec(memory_space=pl.ANY)
        vmem = pl.BlockSpec(memory_space=pltpu.VMEM)
        dma = pltpu.SemaphoreType.DMA
        shapes = (
            ((2, seqs, heads, width, width), BF16),
            ((2, seqs, heads, width), F32),
            ((2, heads, seqs), F32),
            ((seqs, columns // tpn), BF16),
        )
        held = pl.pallas_call(
            functools.partial(kernel, n, tpn),
            out_shape=tuple(pltpu.VMEM(*shape) for shape in shapes),
            in_specs=[any_] * 9,
            out_specs=(vmem,) * 4,
            scratch_shapes=[
                pltpu.VMEM((n * seqs, block, depth), BF16),
                pltpu.VMEM((depth, 2 * width), BF16),
                pltpu.VMEM((width, columns), BF16),
                pltpu.VMEM((2, depth), BF16),
                pltpu.VMEM((2, depth), BF16),
                pltpu.VMEM((1, 2), F32),
                pltpu.VMEM((1, 2), F32),
                pltpu.VMEM((seqs, width), BF16),
                pltpu.VMEM((16, depth), BF16),
                pltpu.VMEM((half, rows, 2 * width), BF16),
                pltpu.VMEM((half, rows, 2 * width), BF16),
                pltpu.VMEM((half, rows, 2 * width), BF16),
                pltpu.VMEM((n, 8, rows), F32),
                pltpu.VMEM((n, 8, rows), F32),
                pltpu.VMEM((seqs, half, block, depth), BF16),
                pltpu.VMEM((4, seqs, half, block, width), F32),
                pltpu.VMEM((seqs, width, width), F32),
                pltpu.VMEM((seqs, width, 2 * width), F32),
                pltpu.VMEM((2, seqs, width), F32),
                pltpu.VMEM((2, seqs, width), F32),
                pltpu.VMEM((tpn, seqs, columns // tpn), F32),
                pltpu.VMEM((tpn, seqs, columns // tpn), F32),
                dma((8,)),
                dma((half + 1,)),
                dma((half,)),
                dma((half,)),
                dma((half,)),
                dma((half,)),
                dma((n,)),
                dma((n,)),
                dma((chips, half)),
                dma((chips, half)),
                dma((chips, half)),
                dma((chips, half)),
                dma((tpn,)),
                dma((tpn,)),
            ],
            compiler_params=pltpu.CompilerParams(collective_id=0, has_side_effects=True),
            name="memories",
        )(
            prompt, w_key.reshape(depth, width), w_value.reshape(depth, width), wo,
            w_in_gate.reshape(2, depth), w_forget_gate.reshape(2, depth),
            in_bias.reshape(1, 2), forget_bias.reshape(1, 2), query.reshape(seqs, width),
        )
        memory, normal, stable, read = pl.pallas_call(
            functools.partial(publish, len(shapes)),
            out_shape=tuple(jax.ShapeDtypeStruct(*shape) for shape in shapes),
            in_specs=[vmem] * len(shapes),
            out_specs=(any_,) * len(shapes),
            scratch_shapes=[dma((len(shapes),))],
            name="outputs",
        )(*[pltpu.with_memory_space_constraint(a, pltpu.VMEM) for a in held])
        return memory, normal, stable.transpose(0, 2, 1), read

    return jax.shard_map(
        body,
        mesh=mesh,
        in_specs=(
            P("gr", "sp", None),
            P(None, "tp", None),
            P(None, "tp", None),
            P(None, None, "tp"),
            P(None, None, "tp"),
            P(None, "tp"),
            P(None, "tp"),
            P(("gr", "sp"), "tp", None),
            P("tp", None, None),
        ),
        out_specs=(
            P(None, ("gr", "sp"), "tp", None, None),
            P(None, ("gr", "sp"), "tp", None),
            P(None, ("gr", "sp"), "tp"),
            P(("gr", "sp"), "tp"),
        ),
        check_vma=False,
    )
```

```python
import functools

import jax
import jax.numpy as jnp
from jax import lax
from jax.experimental import pallas as pl
from jax.experimental.pallas import tpu as pltpu
from jax.sharding import PartitionSpec as P

MESH = pl.DeviceIdType.MESH
F32 = jnp.float32
BF16 = jnp.bfloat16
HIGHEST = lax.Precision.HIGHEST


def nt(a, b):
    return lax.dot_general(a, b, (((1,), (1,)), ((), ())), preferred_element_type=F32)


def tn(a, b):
    return lax.dot_general(a, b, (((0,), (0,)), ((), ())), preferred_element_type=F32)


def iota(shape, axis):
    return lax.broadcasted_iota(jnp.int32, shape, axis)


def kernel(
    n, tpn,
    prompt, wk_hbm, wv_hbm, wo_hbm, ig_hbm, fg_hbm, ib_hbm, fb_hbm, q_hbm,
    membuf, norm_out, stab_out, read_out,
    xall, wkv, wo, in_gate, forget_gate, in_bias, forget_bias, query,
    wg, kvs, kvn, kvf, gsend, grecv, xfar, cols, wb, qb, acc, num, nrm, parts, got,
    lsem, frecv, xrecv, drecv, recv, sent,
):
    sp = lax.axis_index("sp")
    tp = lax.axis_index("tp")
    half = n // 2
    cores = 2
    chips = tpn // cores
    seqs, _, block, depth = xfar.shape
    rows = seqs * block
    width = wo.shape[0]
    line = half // 2
    side = sp // half
    local = sp - side * half
    deck, y = local // line, lax.rem(local, line)
    edge = deck == side
    near_base = side * half
    far_base = half - near_base
    x, c = tp // cores, lax.rem(tp, cores)
    partner = x * cores + 1 - c

    barrier = pltpu.get_barrier_semaphore()
    for k in range(1, n):
        pl.semaphore_signal(
            barrier, inc=1, device_id={"sp": lax.rem(sp + k, n)}, device_id_type=MESH
        )
    for j in range(1, tpn):
        pl.semaphore_signal(
            barrier, inc=1, device_id={"tp": lax.rem(tp + j, tpn)}, device_id_type=MESH
        )

    def far_from(k):
        deck_of = side if k < line else 1 - side
        return deck_of * line + lax.rem(y + line - k % line, line)

    def far_to(i):
        deck_of = 1 - side if i % 2 else side
        return far_base + deck_of * line + lax.rem(y + i // 2, line)

    def near_to(k):
        deck_of = 1 - deck if k < line else deck
        turn = k if k < line else k + 1
        return near_base + deck_of * line + lax.rem(y + turn, line)

    def load(i):
        base = near_base if i == 0 else far_base
        part = pl.ds(base * seqs, half * seqs)
        return pltpu.make_async_copy(prompt.at[part], xall.at[part], lsem.at[i])

    gate_loads = [
        pltpu.make_async_copy(ig_hbm, in_gate, lsem.at[2]),
        pltpu.make_async_copy(fg_hbm, forget_gate, lsem.at[3]),
    ]
    weight_loads = [
        pltpu.make_async_copy(wk_hbm, wkv.at[:, :width], lsem.at[4]),
        pltpu.make_async_copy(wv_hbm, wkv.at[:, width:], lsem.at[5]),
    ]
    late_loads = [
        pltpu.make_async_copy(ib_hbm, in_bias, lsem.at[6]),
        pltpu.make_async_copy(fb_hbm, forget_bias, lsem.at[7]),
        pltpu.make_async_copy(q_hbm, query, lsem.at[8]),
        pltpu.make_async_copy(wo_hbm, wo, lsem.at[9]),
    ]

    def arrived(ref, sem):
        pltpu.make_async_copy(ref, ref, sem).wait()

    def send_far(i):
        dest = far_to(i)
        deck_of = jnp.where(edge, 1, 0)
        return pltpu.make_async_remote_copy(
            src_ref=prompt.at[dest * seqs + tp],
            dst_ref=xfar.at[tp, local],
            send_sem=sent.at[0],
            recv_sem=frecv.at[deck_of * line + i // 2],
            device_id={"sp": dest},
            device_id_type=MESH,
        )

    def send_near(k):
        return pltpu.make_async_remote_copy(
            src_ref=kvs.at[k],
            dst_ref=kvn.at[local],
            send_sem=sent.at[1],
            recv_sem=recv.at[0],
            device_id={"sp": near_to(k)},
            device_id_type=MESH,
        )

    def send_gates(k):
        dest = lax.rem(sp + k, n)
        return pltpu.make_async_remote_copy(
            src_ref=gsend.at[dest],
            dst_ref=grecv.at[sp],
            send_sem=sent.at[2],
            recv_sem=recv.at[1],
            device_id={"sp": dest},
            device_id_type=MESH,
        )

    def spread(j, k):
        piece = xfar.at[tp, far_from(k)]
        return pltpu.make_async_remote_copy(
            src_ref=piece,
            dst_ref=piece,
            send_sem=sent.at[3],
            recv_sem=xrecv.at[j, k],
            device_id={"tp": lax.rem(x + j, chips) * cores + c},
            device_id_type=MESH,
        )

    def hand(j, k):
        origin = lax.rem(x + chips - j, chips) * cores + c
        piece = xfar.at[origin, far_from(k)]
        return pltpu.make_async_remote_copy(
            src_ref=piece,
            dst_ref=piece,
            send_sem=sent.at[4],
            recv_sem=drecv.at[k],
            device_id={"tp": partner},
            device_id_type=MESH,
        )

    def give(j):
        peer = lax.rem(tp + j, tpn)
        return pltpu.make_async_remote_copy(
            src_ref=parts.at[peer],
            dst_ref=got.at[j],
            send_sem=sent.at[5],
            recv_sem=recv.at[2],
            device_id={"tp": peer},
            device_id_type=MESH,
        )

    for copy in gate_loads:
        copy.start()
    load(0).start()
    load(1).start()
    for copy in weight_loads + late_loads:
        copy.start()

    for copy in gate_loads:
        copy.wait()
    load(0).wait()
    wg[...] = jnp.concatenate(
        [in_gate[...].astype(F32), forget_gate[...].astype(F32), jnp.zeros((wg.shape[0] - 4, depth), F32)],
        axis=0,
    ).astype(BF16)

    def rows_of(dest):
        return xall[pl.ds(dest * seqs, seqs)].reshape(rows, depth)

    for base in (near_base, far_base):
        if base is far_base:
            load(1).wait()
        for k in range(half):
            gsend[pl.ds(base + k, 1)] = nt(wg[...], rows_of(base + k))[:4][None]
    grecv[pl.ds(sp, 1)] = gsend[pl.ds(sp, 1)]
    pl.semaphore_wait(barrier, n - 1 + tpn - 1)
    for k in range(1, n):
        send_gates(k).start()

    @pl.when(jnp.logical_not(edge))
    def _():
        for i in range(half):
            send_far(i).start()

    for copy in weight_loads:
        copy.wait()
    for k in range(half):
        dest = near_to(k)
        both = jnp.dot(rows_of(dest), wkv[...], preferred_element_type=F32).astype(BF16)
        if k < half - 1:
            kvs[k] = both
            send_near(k).start()
        else:
            kvn[pl.ds(local, 1)] = both[None]
        if k == line - 1:

            @pl.when(edge)
            def _():
                for i in range(half):
                    send_far(i).start()


    def weigh():
        lane = iota((rows, rows), 1)
        down = iota((rows, rows), 0)
        same = (lane // block) == (down // block)
        upto = (same & (down <= lane)).astype(F32)
        whole = same.astype(F32)
        before = (
            (iota((2 * n, 2 * n), 0) // n == iota((2 * n, 2 * n), 1) // n)
            & (iota((2 * n, 2 * n), 1) < iota((2 * n, 2 * n), 0))
        ).astype(F32)
        pre = [
            grecv[:, i, :] + (in_bias if i < 2 else forget_bias)[0:1, i % 2 : i % 2 + 1]
            for i in range(4)
        ]
        forget_pre = jnp.concatenate(pre[2:], axis=0)
        forget = jnp.minimum(forget_pre, 0.0) - jnp.log1p(jnp.exp(-jnp.abs(forget_pre)))
        inside = jnp.dot(forget, upto, preferred_element_type=F32, precision=HIGHEST)
        sums = jnp.dot(forget, whole, preferred_element_type=F32, precision=HIGHEST)
        running = jnp.dot(before, sums, preferred_element_type=F32, precision=HIGHEST) + inside
        totals = [jnp.sum(sums[g * n : (g + 1) * n], axis=0, keepdims=True) for g in range(2)]
        logs = [
            pre[0] + totals[0] - running[:n],
            pre[1] + running[n:] - forget[n:],
        ]
        peak = jnp.concatenate(
            [jnp.maximum(totals[g], jnp.max(logs[g], axis=0, keepdims=True)) for g in range(2)]
            + [jnp.zeros((6, rows), F32)],
            axis=0,
        )
        spot = iota(peak.shape, 1)
        step = 1
        while step < block:
            low, high = pltpu.roll(peak, step, 1), pltpu.roll(peak, rows - step, 1)
            peak = jnp.maximum(peak, jnp.where((spot & step) != 0, low, high))
            step *= 2
        weight = [jnp.exp(logs[g] - peak[g : g + 1]) * width ** (-0.5) for g in range(2)]
        first = side == 0
        parted = [jnp.where(first, w[:half], w[half:]) for w in weight]
        parted += [jnp.where(first, w[half:], w[:half]) for w in weight]
        cols[...] = jnp.concatenate(parted, axis=0).T
        own = iota((seqs, rows), 1) // block == iota((seqs, rows), 0)
        return [
            jnp.max(jnp.where(own, peak[g : g + 1], -jnp.inf), axis=1, keepdims=True)
            for g in range(2)
        ]

    def widen(i):
        for q in range(seqs):
            for s in range(half):
                j = i * half + s
                wb[i, q, s] = jnp.broadcast_to(
                    cols[q * block : (q + 1) * block, j : j + 1], (block, width)
                )

    def outer(kv, i, q):
        lines = slice(q * block, (q + 1) * block)
        keys = kv[:, lines, :width].reshape(half * block, width)
        values = kv[:, lines, width:].reshape(half * block, width).astype(F32)
        w0 = wb[2 * i, q].reshape(half * block, width)
        w1 = wb[2 * i + 1, q].reshape(half * block, width)
        weighted = jnp.concatenate([values * w0, values * w1], axis=1).astype(BF16)
        keys_f = keys.astype(F32)
        sums = [jnp.sum(keys_f * w, axis=0, keepdims=True) for w in (w0, w1)]
        return tn(keys, weighted), sums

    def project(k):
        source = far_from(k)
        lines = xfar[:, pl.ds(source, 1)].reshape(rows, depth)
        kvf[pl.ds(source, 1)] = jnp.dot(
            lines, wkv[...], preferred_element_type=F32
        ).astype(BF16)[None]

    lag_hand, lag_project = 2, 4
    stable = None
    for step in range(half + lag_project):
        if step < half:
            arrived(xfar.at[0, 0], frecv.at[step])
            for j in (2, 1, 3):
                spread(j, step).start()
            hand(0, step).start()
        k = step - lag_hand
        if 0 <= k < half:
            for j in (1, 3, 2):
                arrived(xfar.at[0, 0], xrecv.at[j, k])
                hand(j, k).start()
        if step == 0:
            for copy in late_loads:
                copy.wait()
            turned = query[...].astype(F32).T
            for q in range(seqs):
                qb[q] = jnp.broadcast_to(turned[:, q : q + 1], (width, width))
        if step == 2:
            arrived(grecv.at[pl.ds(0, n - 1)], recv.at[1])
            stable = weigh()
        if step in (3, 4):
            widen(2 * (step - 3))
            widen(2 * (step - 3) + 1)
        if step == half:
            arrived(kvn.at[pl.ds(0, half - 1)], recv.at[0])
            for q in range(seqs):
                acc[q], sums = outer(kvn, 0, q)
                for g in range(2):
                    nrm[g, q : q + 1] = sums[g]
        k = step - lag_project
        if 0 <= k < half:
            arrived(xfar.at[0, pl.ds(0, chips)], drecv.at[k])
            project(k)

    for q in range(seqs):
        more, sums = outer(kvf, 1, q)
        memory = (acc[q] + more).astype(BF16)
        back = memory.astype(F32)
        for g in range(2):
            membuf[g, q, 0] = memory[:, g * width : (g + 1) * width]
            num[g, q : q + 1] = jnp.sum(
                qb[q] * back[:, g * width : (g + 1) * width], axis=0, keepdims=True
            )
            total = nrm[g, q : q + 1] + sums[g]
            nrm[g, q : q + 1] = total
            norm_out[g, q] = total

    hidden = jnp.zeros((seqs, width), F32)
    queries = query[...].astype(F32)
    for g in range(2):
        under = jnp.abs(jnp.sum(queries * nrm[g], axis=1, keepdims=True))
        floor = jnp.maximum(jnp.exp(-stable[g]), 1.0)
        hidden = hidden + num[g] / jnp.maximum(under, floor)
        square = iota((seqs, width), 1) == iota((seqs, width), 0)
        row = jnp.sum(jnp.where(square, stable[g], 0.0), axis=0, keepdims=True)
        stab_out[g] = row[:, :seqs]
    terms = jnp.dot(hidden.astype(BF16), wo[...], preferred_element_type=F32)
    share = terms.shape[1] // tpn
    for t in range(tpn):
        parts[t] = terms[:, t * share : (t + 1) * share]
    for j in range(1, tpn):
        give(j).start()
    arrived(xfar.at[0], sent.at[0])
    arrived(kvn.at[pl.ds(0, half - 1)], sent.at[1])
    arrived(grecv.at[pl.ds(0, n - 1)], sent.at[2])
    arrived(xfar.at[pl.ds(0, chips - 1)], sent.at[3])
    arrived(xfar.at[pl.ds(0, chips)], sent.at[4])
    arrived(got.at[pl.ds(0, tpn - 1)], sent.at[5])
    arrived(got.at[pl.ds(0, tpn - 1)], recv.at[2])
    total = parts[tp]
    for j in range(1, tpn):
        total = total + got[j]
    read_out[...] = total.astype(BF16)


def publish(count, *refs):
    sources, targets, sems = refs[:count], refs[count : 2 * count], refs[2 * count]
    copies = [
        pltpu.make_async_copy(a, b, sems.at[i]) for i, (a, b) in enumerate(zip(sources, targets))
    ]
    for copy in copies:
        copy.start()
    for copy in copies:
        copy.wait()


def solution(mesh):
    n, tpn = mesh.shape["sp"], mesh.shape["tp"]

    def body(prompt, w_key, w_value, w_in_gate, w_forget_gate, in_bias, forget_bias, query, w_out):
        depth, heads, width = w_key.shape
        seqs = prompt.shape[0] // n
        block = prompt.shape[1]
        rows = seqs * block
        half = n // 2
        chips = tpn // 2
        wo = w_out.reshape(heads * width, -1)
        columns = wo.shape[1]
        any_ = pl.BlockSpec(memory_space=pl.ANY)
        vmem = pl.BlockSpec(memory_space=pltpu.VMEM)
        dma = pltpu.SemaphoreType.DMA
        shapes = (
            ((2, seqs, heads, width, width), BF16),
            ((2, seqs, heads, width), F32),
            ((2, heads, seqs), F32),
            ((seqs, columns // tpn), BF16),
        )
        held = pl.pallas_call(
            functools.partial(kernel, n, tpn),
            out_shape=tuple(pltpu.VMEM(*shape) for shape in shapes),
            in_specs=[any_] * 9,
            out_specs=(vmem,) * 4,
            scratch_shapes=[
                pltpu.VMEM((n * seqs, block, depth), BF16),
                pltpu.VMEM((depth, 2 * width), BF16),
                pltpu.VMEM((width, columns), BF16),
                pltpu.VMEM((2, depth), BF16),
                pltpu.VMEM((2, depth), BF16),
                pltpu.VMEM((1, 2), F32),
                pltpu.VMEM((1, 2), F32),
                pltpu.VMEM((seqs, width), BF16),
                pltpu.VMEM((16, depth), BF16),
                pltpu.VMEM((half, rows, 2 * width), BF16),
                pltpu.VMEM((half, rows, 2 * width), BF16),
                pltpu.VMEM((half, rows, 2 * width), BF16),
                pltpu.VMEM((n, 4, rows), F32),
                pltpu.VMEM((n, 4, rows), F32),
                pltpu.VMEM((seqs, half, block, depth), BF16),
                pltpu.VMEM((rows, 4 * half), F32),
                pltpu.VMEM((4, seqs, half, block, width), F32),
                pltpu.VMEM((seqs, width, width), F32),
                pltpu.VMEM((seqs, width, 2 * width), F32),
                pltpu.VMEM((2, seqs, width), F32),
                pltpu.VMEM((2, seqs, width), F32),
                pltpu.VMEM((tpn, seqs, columns // tpn), F32),
                pltpu.VMEM((tpn, seqs, columns // tpn), F32),
                dma((10,)),
                dma((half,)),
                dma((chips, half)),
                dma((half,)),
                dma((3,)),
                dma((6,)),
            ],
            compiler_params=pltpu.CompilerParams(collective_id=0, has_side_effects=True),
            name="memories",
        )(
            prompt, w_key.reshape(depth, width), w_value.reshape(depth, width), wo,
            w_in_gate.reshape(2, depth), w_forget_gate.reshape(2, depth),
            in_bias.reshape(1, 2), forget_bias.reshape(1, 2), query.reshape(seqs, width),
        )
        memory, normal, stable, read = pl.pallas_call(
            functools.partial(publish, len(shapes)),
            out_shape=tuple(jax.ShapeDtypeStruct(*shape) for shape in shapes),
            in_specs=[vmem] * len(shapes),
            out_specs=(any_,) * len(shapes),
            scratch_shapes=[dma((len(shapes),))],
            name="outputs",
        )(*[pltpu.with_memory_space_constraint(a, pltpu.VMEM) for a in held])
        return memory, normal, stable.transpose(0, 2, 1), read

    return jax.shard_map(
        body,
        mesh=mesh,
        in_specs=(
            P("gr", "sp", None),
            P(None, "tp", None),
            P(None, "tp", None),
            P(None, None, "tp"),
            P(None, None, "tp"),
            P(None, "tp"),
            P(None, "tp"),
            P(("gr", "sp"), "tp", None),
            P("tp", None, None),
        ),
        out_specs=(
            P(None, ("gr", "sp"), "tp", None, None),
            P(None, ("gr", "sp"), "tp", None),
            P(None, ("gr", "sp"), "tp"),
            P(("gr", "sp"), "tp"),
        ),
        check_vma=False,
    )
```

```python
import functools

import jax
import jax.numpy as jnp
from jax import lax
from jax.experimental import pallas as pl
from jax.experimental.pallas import tpu as pltpu
from jax.sharding import PartitionSpec as P

MESH = pl.DeviceIdType.MESH
F32 = jnp.float32
BF16 = jnp.bfloat16
HIGHEST = lax.Precision.HIGHEST


def nt(a, b):
    return lax.dot_general(a, b, (((1,), (1,)), ((), ())), preferred_element_type=F32)


def tn(a, b):
    return lax.dot_general(a, b, (((0,), (0,)), ((), ())), preferred_element_type=F32)


def iota(shape, axis):
    return lax.broadcasted_iota(jnp.int32, shape, axis)


NEAR_ORDER = (0, 1, 4, "far", 2, 5, 3, 6)


def kernel(
    n, tpn,
    prompt, wk_hbm, wv_hbm, wo_hbm, ig_hbm, fg_hbm, ib_hbm, fb_hbm, q_hbm,
    membuf, norm_out, stab_out, read_out,
    xall, wkv, wo, in_gate, forget_gate, in_bias, forget_bias, query,
    wg, kvs, kvn, kvf, gsend, grecv, xfar, cols, wb, qb, acc, num, nrm, parts, got,
    lsem, frecv, xrecv, drecv, recv, sent,
):
    sp = lax.axis_index("sp")
    tp = lax.axis_index("tp")
    half = n // 2
    cores = 2
    chips = tpn // cores
    seqs, _, block, depth = xfar.shape
    rows = seqs * block
    width = wo.shape[0]
    line = half // 2
    side = sp // half
    local = sp - side * half
    deck, y = local // line, lax.rem(local, line)
    edge = deck == side
    near_base = side * half
    far_base = half - near_base
    x, c = tp // cores, lax.rem(tp, cores)
    partner = x * cores + 1 - c

    barrier = pltpu.get_barrier_semaphore()
    for k in range(1, n):
        pl.semaphore_signal(
            barrier, inc=1, device_id={"sp": lax.rem(sp + k, n)}, device_id_type=MESH
        )
    for j in range(1, tpn):
        pl.semaphore_signal(
            barrier, inc=1, device_id={"tp": lax.rem(tp + j, tpn)}, device_id_type=MESH
        )

    turns = line - 1
    steps = 2 * turns

    def far_from(k):
        deck_of = 1 - side if k < turns else side
        return deck_of * line + lax.rem(y + line - 1 - k % turns, line)

    def far_to(i):
        deck_of = 1 - side if i % 2 else side
        return far_base + deck_of * line + lax.rem(y + 1 + i // 2, line)

    def near_to(k):
        deck_of = 1 - deck if k < line else deck
        turn = k if k < line else k + 1
        return near_base + deck_of * line + lax.rem(y + turn, line)

    pieces = 4

    def load(i):
        base = (near_base if i < pieces // 2 else far_base) + i % (pieces // 2) * (2 * half // pieces)
        part = pl.ds(base * seqs, 2 * half // pieces * seqs)
        return pltpu.make_async_copy(prompt.at[part], xall.at[part], lsem.at[i])

    gate_loads = [
        pltpu.make_async_copy(ig_hbm, in_gate, lsem.at[4]),
        pltpu.make_async_copy(fg_hbm, forget_gate, lsem.at[5]),
    ]
    weight_loads = [
        pltpu.make_async_copy(wk_hbm, wkv.at[:, :width], lsem.at[6]),
        pltpu.make_async_copy(wv_hbm, wkv.at[:, width:], lsem.at[7]),
    ]
    late_loads = [
        pltpu.make_async_copy(ib_hbm, in_bias, lsem.at[8]),
        pltpu.make_async_copy(fb_hbm, forget_bias, lsem.at[9]),
        pltpu.make_async_copy(q_hbm, query, lsem.at[10]),
        pltpu.make_async_copy(wo_hbm, wo, lsem.at[11]),
    ]

    def arrived(ref, sem):
        pltpu.make_async_copy(ref, ref, sem).wait()

    def send_far(i):
        dest = far_to(i)
        late = jnp.where(edge, 0, turns)
        return pltpu.make_async_remote_copy(
            src_ref=prompt.at[dest * seqs + tp],
            dst_ref=xfar.at[tp, local],
            send_sem=sent.at[0],
            recv_sem=frecv.at[late + i // 2],
            device_id={"sp": dest},
            device_id_type=MESH,
        )

    def send_near(k):
        return pltpu.make_async_remote_copy(
            src_ref=kvs.at[k],
            dst_ref=kvn.at[local],
            send_sem=sent.at[1],
            recv_sem=recv.at[0],
            device_id={"sp": near_to(k)},
            device_id_type=MESH,
        )

    def send_line(i):
        return pltpu.make_async_remote_copy(
            src_ref=kvs.at[half - 1 + i],
            dst_ref=kvf.at[local],
            send_sem=sent.at[1],
            recv_sem=recv.at[3],
            device_id={"sp": far_base + i * line + y},
            device_id_type=MESH,
        )

    def send_gates(k):
        dest = lax.rem(sp + k, n)
        return pltpu.make_async_remote_copy(
            src_ref=gsend.at[dest],
            dst_ref=grecv.at[sp],
            send_sem=sent.at[2],
            recv_sem=recv.at[1],
            device_id={"sp": dest},
            device_id_type=MESH,
        )

    def spread(j, k):
        piece = xfar.at[tp, far_from(k)]
        return pltpu.make_async_remote_copy(
            src_ref=piece,
            dst_ref=piece,
            send_sem=sent.at[3],
            recv_sem=xrecv.at[j, k],
            device_id={"tp": lax.rem(x + j, chips) * cores + c},
            device_id_type=MESH,
        )

    def hand(j, k):
        origin = lax.rem(x + chips - j, chips) * cores + c
        piece = xfar.at[origin, far_from(k)]
        return pltpu.make_async_remote_copy(
            src_ref=piece,
            dst_ref=piece,
            send_sem=sent.at[4],
            recv_sem=drecv.at[k],
            device_id={"tp": partner},
            device_id_type=MESH,
        )

    def give(j):
        peer = lax.rem(tp + j, tpn)
        return pltpu.make_async_remote_copy(
            src_ref=parts.at[peer],
            dst_ref=got.at[j],
            send_sem=sent.at[5],
            recv_sem=recv.at[2],
            device_id={"tp": peer},
            device_id_type=MESH,
        )

    for copy in gate_loads:
        copy.start()
    for i in range(pieces):
        load(i).start()
    for copy in weight_loads + late_loads:
        copy.start()

    for copy in gate_loads:
        copy.wait()
    wg[...] = jnp.concatenate(
        [in_gate[...].astype(F32), forget_gate[...].astype(F32), jnp.zeros((wg.shape[0] - 4, depth), F32)],
        axis=0,
    ).astype(BF16)

    def rows_of(dest):
        return xall[pl.ds(dest * seqs, seqs)].reshape(rows, depth)

    def gates(start, stop):
        for i in range(start, stop):
            if i % (2 * half // pieces) == 0:
                load(i // (2 * half // pieces)).wait()
            dest = (near_base if i < half else far_base) + i % half
            gsend[pl.ds(dest, 1)] = nt(wg[...], rows_of(dest))[:4][None]

    gates(0, half)
    pl.semaphore_wait(barrier, n - 1 + tpn - 1)
    inner = jnp.logical_not(edge)

    @pl.when(edge)
    def _():
        for i in range(steps):
            send_far(i).start()

    gates(half, 2 * half)
    grecv[pl.ds(sp, 1)] = gsend[pl.ds(sp, 1)]
    for k in range(1, n):
        send_gates(k).start()
    for copy in weight_loads:
        copy.wait()

    def keys_values(dest):
        return jnp.dot(rows_of(dest), wkv[...], preferred_element_type=F32).astype(BF16)

    for k in NEAR_ORDER:
        if k == "far":

            @pl.when(inner)
            def _():
                for i in range(steps):
                    send_far(i).start()

            continue
        kvs[k] = keys_values(near_to(k))
        send_near(k).start()
    for i in range(2):
        kvs[half - 1 + i] = keys_values(far_base + i * line + y)
        send_line(i).start()
    kvn[pl.ds(local, 1)] = keys_values(near_to(half - 1))[None]

    def weigh():
        lane = iota((rows, rows), 1)
        down = iota((rows, rows), 0)
        same = (lane // block) == (down // block)
        upto = (same & (down <= lane)).astype(F32)
        whole = same.astype(F32)
        before = (
            (iota((2 * n, 2 * n), 0) // n == iota((2 * n, 2 * n), 1) // n)
            & (iota((2 * n, 2 * n), 1) < iota((2 * n, 2 * n), 0))
        ).astype(F32)
        pre = [
            grecv[:, i, :] + (in_bias if i < 2 else forget_bias)[0:1, i % 2 : i % 2 + 1]
            for i in range(4)
        ]
        forget_pre = jnp.concatenate(pre[2:], axis=0)
        forget = jnp.minimum(forget_pre, 0.0) - jnp.log1p(jnp.exp(-jnp.abs(forget_pre)))
        inside = jnp.dot(forget, upto, preferred_element_type=F32, precision=HIGHEST)
        sums = jnp.dot(forget, whole, preferred_element_type=F32, precision=HIGHEST)
        running = jnp.dot(before, sums, preferred_element_type=F32, precision=HIGHEST) + inside
        totals = [jnp.sum(sums[g * n : (g + 1) * n], axis=0, keepdims=True) for g in range(2)]
        logs = [
            pre[0] + totals[0] - running[:n],
            pre[1] + running[n:] - forget[n:],
        ]
        peak = jnp.concatenate(
            [jnp.maximum(totals[g], jnp.max(logs[g], axis=0, keepdims=True)) for g in range(2)]
            + [jnp.zeros((6, rows), F32)],
            axis=0,
        )
        spot = iota(peak.shape, 1)
        step = 1
        while step < block:
            low, high = pltpu.roll(peak, step, 1), pltpu.roll(peak, rows - step, 1)
            peak = jnp.maximum(peak, jnp.where((spot & step) != 0, low, high))
            step *= 2
        weight = [jnp.exp(logs[g] - peak[g : g + 1]) * width ** (-0.5) for g in range(2)]
        first = side == 0
        parted = [jnp.where(first, w[:half], w[half:]) for w in weight]
        parted += [jnp.where(first, w[half:], w[:half]) for w in weight]
        cols[...] = jnp.concatenate(parted, axis=0).T
        own = iota((seqs, rows), 1) // block == iota((seqs, rows), 0)
        return [
            jnp.max(jnp.where(own, peak[g : g + 1], -jnp.inf), axis=1, keepdims=True)
            for g in range(2)
        ]

    def widen(i):
        for q in range(seqs):
            for s in range(half):
                j = i * half + s
                wb[i, q, s] = jnp.broadcast_to(
                    cols[q * block : (q + 1) * block, j : j + 1], (block, width)
                )

    def outer(kv, i, q):
        lines = slice(q * block, (q + 1) * block)
        keys = kv[:, lines, :width].reshape(half * block, width)
        values = kv[:, lines, width:].reshape(half * block, width).astype(F32)
        w0 = wb[2 * i, q].reshape(half * block, width)
        w1 = wb[2 * i + 1, q].reshape(half * block, width)
        weighted = jnp.concatenate([values * w0, values * w1], axis=1).astype(BF16)
        keys_f = keys.astype(F32)
        sums = [jnp.sum(keys_f * w, axis=0, keepdims=True) for w in (w0, w1)]
        return tn(keys, weighted), sums

    def project(p):
        found = [far_from(2 * p), far_from(2 * p + 1)]
        lines = [xfar[:, pl.ds(source, 1)].reshape(rows, depth) for source in found]
        both = jnp.dot(
            jnp.concatenate(lines, axis=0), wkv[...], preferred_element_type=F32
        ).astype(BF16)
        for i, source in enumerate(found):
            kvf[pl.ds(source, 1)] = both[i * rows : (i + 1) * rows][None]

    def own(p):
        for k in (2 * p, 2 * p + 1):
            arrived(xfar.at[0, 0], frecv.at[k])
            for j in (2, 1, 3):
                spread(j, k).start()
            hand(0, k).start()

    def pass_on(p):
        for k in (2 * p, 2 * p + 1):
            for j in (1, 3, 2):
                arrived(xfar.at[0, 0], xrecv.at[j, k])
                hand(j, k).start()

    def collect(p):
        for k in (2 * p, 2 * p + 1):
            arrived(xfar.at[0, pl.ds(0, chips)], drecv.at[k])
        project(p)

    own(0)
    for copy in late_loads:
        copy.wait()
    turned = query[...].astype(F32).T
    for q in range(seqs):
        qb[q] = jnp.broadcast_to(turned[:, q : q + 1], (width, width))
    arrived(grecv.at[pl.ds(0, n - 1)], recv.at[1])
    stable = weigh()
    own(1)
    widen(0)
    widen(1)
    pass_on(0)
    own(2)
    widen(2)
    widen(3)
    pass_on(1)
    collect(0)
    pass_on(2)
    arrived(kvn.at[pl.ds(0, half - 1)], recv.at[0])
    for q in range(seqs):
        acc[q], sums = outer(kvn, 0, q)
        for g in range(2):
            nrm[g, q : q + 1] = sums[g]
    collect(1)
    collect(2)
    arrived(kvf.at[pl.ds(0, 2)], recv.at[3])
    for q in range(seqs):
        more, sums = outer(kvf, 1, q)
        memory = (acc[q] + more).astype(BF16)
        back = memory.astype(F32)
        for g in range(2):
            membuf[g, q, 0] = memory[:, g * width : (g + 1) * width]
            num[g, q : q + 1] = jnp.sum(
                qb[q] * back[:, g * width : (g + 1) * width], axis=0, keepdims=True
            )
            total = nrm[g, q : q + 1] + sums[g]
            nrm[g, q : q + 1] = total
            norm_out[g, q] = total

    hidden = jnp.zeros((seqs, width), F32)
    queries = query[...].astype(F32)
    for g in range(2):
        under = jnp.abs(jnp.sum(queries * nrm[g], axis=1, keepdims=True))
        floor = jnp.maximum(jnp.exp(-stable[g]), 1.0)
        hidden = hidden + num[g] / jnp.maximum(under, floor)
        square = iota((seqs, width), 1) == iota((seqs, width), 0)
        row = jnp.sum(jnp.where(square, stable[g], 0.0), axis=0, keepdims=True)
        stab_out[g] = row[:, :seqs]
    terms = jnp.dot(hidden.astype(BF16), wo[...], preferred_element_type=F32)
    share = terms.shape[1] // tpn
    for t in range(tpn):
        parts[t] = terms[:, t * share : (t + 1) * share]
    for j in range(1, tpn):
        give(j).start()
    arrived(xfar.at[0, pl.ds(0, steps)], sent.at[0])
    arrived(kvs, sent.at[1])
    arrived(grecv.at[pl.ds(0, n - 1)], sent.at[2])
    arrived(xfar.at[pl.ds(0, chips - 1), pl.ds(0, steps)], sent.at[3])
    arrived(xfar.at[pl.ds(0, chips), pl.ds(0, steps)], sent.at[4])
    arrived(got.at[pl.ds(0, tpn - 1)], sent.at[5])
    arrived(got.at[pl.ds(0, tpn - 1)], recv.at[2])
    total = parts[tp]
    for j in range(1, tpn):
        total = total + got[j]
    read_out[...] = total.astype(BF16)


def publish(count, *refs):
    sources, targets, sems = refs[:count], refs[count : 2 * count], refs[2 * count]
    copies = [
        pltpu.make_async_copy(a, b, sems.at[i]) for i, (a, b) in enumerate(zip(sources, targets))
    ]
    for copy in copies:
        copy.start()
    for copy in copies:
        copy.wait()


def solution(mesh):
    n, tpn = mesh.shape["sp"], mesh.shape["tp"]

    def body(prompt, w_key, w_value, w_in_gate, w_forget_gate, in_bias, forget_bias, query, w_out):
        depth, heads, width = w_key.shape
        seqs = prompt.shape[0] // n
        block = prompt.shape[1]
        rows = seqs * block
        half = n // 2
        chips = tpn // 2
        steps = 2 * (half // 2 - 1)
        wo = w_out.reshape(heads * width, -1)
        columns = wo.shape[1]
        any_ = pl.BlockSpec(memory_space=pl.ANY)
        vmem = pl.BlockSpec(memory_space=pltpu.VMEM)
        dma = pltpu.SemaphoreType.DMA
        shapes = (
            ((2, seqs, heads, width, width), BF16),
            ((2, seqs, heads, width), F32),
            ((2, heads, seqs), F32),
            ((seqs, columns // tpn), BF16),
        )
        held = pl.pallas_call(
            functools.partial(kernel, n, tpn),
            out_shape=tuple(pltpu.VMEM(*shape) for shape in shapes),
            in_specs=[any_] * 9,
            out_specs=(vmem,) * 4,
            scratch_shapes=[
                pltpu.VMEM((n * seqs, block, depth), BF16),
                pltpu.VMEM((depth, 2 * width), BF16),
                pltpu.VMEM((width, columns), BF16),
                pltpu.VMEM((2, depth), BF16),
                pltpu.VMEM((2, depth), BF16),
                pltpu.VMEM((1, 2), F32),
                pltpu.VMEM((1, 2), F32),
                pltpu.VMEM((seqs, width), BF16),
                pltpu.VMEM((16, depth), BF16),
                pltpu.VMEM((half + 1, rows, 2 * width), BF16),
                pltpu.VMEM((half, rows, 2 * width), BF16),
                pltpu.VMEM((half, rows, 2 * width), BF16),
                pltpu.VMEM((n, 4, rows), F32),
                pltpu.VMEM((n, 4, rows), F32),
                pltpu.VMEM((seqs, half, block, depth), BF16),
                pltpu.VMEM((rows, 4 * half), F32),
                pltpu.VMEM((4, seqs, half, block, width), F32),
                pltpu.VMEM((seqs, width, width), F32),
                pltpu.VMEM((seqs, width, 2 * width), F32),
                pltpu.VMEM((2, seqs, width), F32),
                pltpu.VMEM((2, seqs, width), F32),
                pltpu.VMEM((tpn, seqs, columns // tpn), F32),
                pltpu.VMEM((tpn, seqs, columns // tpn), F32),
                dma((12,)),
                dma((steps,)),
                dma((chips, steps)),
                dma((steps,)),
                dma((4,)),
                dma((6,)),
            ],
            compiler_params=pltpu.CompilerParams(collective_id=0, has_side_effects=True),
            name="memories",
        )(
            prompt, w_key.reshape(depth, width), w_value.reshape(depth, width), wo,
            w_in_gate.reshape(2, depth), w_forget_gate.reshape(2, depth),
            in_bias.reshape(1, 2), forget_bias.reshape(1, 2), query.reshape(seqs, width),
        )
        memory, normal, stable, read = pl.pallas_call(
            functools.partial(publish, len(shapes)),
            out_shape=tuple(jax.ShapeDtypeStruct(*shape) for shape in shapes),
            in_specs=[vmem] * len(shapes),
            out_specs=(any_,) * len(shapes),
            scratch_shapes=[dma((len(shapes),))],
            name="outputs",
        )(*[pltpu.with_memory_space_constraint(a, pltpu.VMEM) for a in held])
        return memory, normal, stable.transpose(0, 2, 1), read

    return jax.shard_map(
        body,
        mesh=mesh,
        in_specs=(
            P("gr", "sp", None),
            P(None, "tp", None),
            P(None, "tp", None),
            P(None, None, "tp"),
            P(None, None, "tp"),
            P(None, "tp"),
            P(None, "tp"),
            P(("gr", "sp"), "tp", None),
            P("tp", None, None),
        ),
        out_specs=(
            P(None, ("gr", "sp"), "tp", None, None),
            P(None, ("gr", "sp"), "tp", None),
            P(None, ("gr", "sp"), "tp"),
            P(("gr", "sp"), "tp"),
        ),
        check_vma=False,
    )
```

```python
import functools

import jax
import jax.numpy as jnp
from jax import lax
from jax.experimental import pallas as pl
from jax.experimental.pallas import tpu as pltpu
from jax.sharding import PartitionSpec as P

MESH = pl.DeviceIdType.MESH
F32 = jnp.float32
BF16 = jnp.bfloat16
HIGHEST = lax.Precision.HIGHEST


def nt(a, b):
    return lax.dot_general(a, b, (((1,), (1,)), ((), ())), preferred_element_type=F32)


def tn(a, b):
    return lax.dot_general(a, b, (((0,), (0,)), ((), ())), preferred_element_type=F32)


def iota(shape, axis):
    return lax.broadcasted_iota(jnp.int32, shape, axis)


NEAR_ORDER = ("far", 0, 1, 4, 2, 5, 3, 6)
ORDER = (
    ("own", 0),
    ("own", 1),
    ("queries", 0),
    ("own", 2),
    ("own", 3),
    ("pass", 0),
    ("own", 4),
    ("own", 5),
    ("pass", 1),
    ("gates", 0),
    ("pass", 2),
    ("widen", 0),
    ("widen", 1),
    ("pass", 3),
    ("widen", 2),
    ("widen", 3),
    ("collect", 0),
    ("near", 0),
    ("pass", 4),
    ("collect", 1),
    ("pass", 5),
    ("collect", 2),
)


def kernel(
    n, tpn,
    prompt, wk_hbm, wv_hbm, wo_hbm, ig_hbm, fg_hbm, ib_hbm, fb_hbm, q_hbm,
    membuf, norm_out, stab_out, read_out,
    xall, wkv, wo, gate_w, biases, query,
    wg, kvs, kvn, kvf, gsend, grecv, xfar, cols, wb, qb, acc, num, nrm, parts, got,
    lsem, frecv, xrecv, drecv, recv, sent,
):
    sp = lax.axis_index("sp")
    tp = lax.axis_index("tp")
    half = n // 2
    cores = 2
    chips = tpn // cores
    seqs, _, block, depth = xfar.shape
    rows = seqs * block
    width = wo.shape[0]
    line = half // 2
    side = sp // half
    local = sp - side * half
    deck, y = local // line, lax.rem(local, line)
    edge = deck == side
    near_base = side * half
    far_base = half - near_base
    x, c = tp // cores, lax.rem(tp, cores)
    partner = x * cores + 1 - c

    barrier = pltpu.get_barrier_semaphore()
    for i in range(half):
        pl.semaphore_signal(
            barrier,
            inc=1,
            device_id={"sp": far_base + lax.rem(local + half // 2 + i, half)},
            device_id_type=MESH,
        )
    for k in range(1, half):
        pl.semaphore_signal(
            barrier,
            inc=1,
            device_id={"sp": near_base + lax.rem(local + k, half)},
            device_id_type=MESH,
        )
    for j in range(1, tpn):
        pl.semaphore_signal(
            barrier, inc=1, device_id={"tp": lax.rem(tp + j, tpn)}, device_id_type=MESH
        )

    turns = line - 1
    steps = 2 * turns

    def turn_of(i):
        return (line // 2, 1, line - 1)[i]

    def far_from(k):
        deck_of = 1 - side if k < turns else side
        return deck_of * line + lax.rem(y + line - turn_of(k % turns), line)

    def far_to(i):
        deck_of = 1 - side if i < turns else side
        return far_base + deck_of * line + lax.rem(y + turn_of(i % turns), line)

    def near_to(k):
        deck_of = 1 - deck if k < line else deck
        turn = k if k < line else k + 1
        return near_base + deck_of * line + lax.rem(y + turn, line)

    pieces = 4

    def load(i):
        base = (near_base if i < pieces // 2 else far_base) + i % (pieces // 2) * (2 * half // pieces)
        part = pl.ds(base * seqs, 2 * half // pieces * seqs)
        return pltpu.make_async_copy(prompt.at[part], xall.at[part], lsem.at[i])

    gate_loads = [
        pltpu.make_async_copy(ig_hbm, gate_w.at[0], lsem.at[4]),
        pltpu.make_async_copy(fg_hbm, gate_w.at[1], lsem.at[4]),
    ]
    weight_loads = [
        pltpu.make_async_copy(wk_hbm, wkv.at[:, :width], lsem.at[5]),
        pltpu.make_async_copy(wv_hbm, wkv.at[:, width:], lsem.at[5]),
    ]
    late_loads = [
        pltpu.make_async_copy(ib_hbm, biases.at[0], lsem.at[6]),
        pltpu.make_async_copy(fb_hbm, biases.at[1], lsem.at[6]),
        pltpu.make_async_copy(q_hbm, query, lsem.at[7]),
        pltpu.make_async_copy(wo_hbm, wo, lsem.at[8]),
    ]

    def arrived(ref, sem):
        pltpu.make_async_copy(ref, ref, sem).wait()

    def send_far(i):
        dest = far_to(i)
        late = jnp.where(edge, 0, turns)
        return pltpu.make_async_remote_copy(
            src_ref=xall.at[dest * seqs + tp],
            dst_ref=xfar.at[tp, local],
            send_sem=sent.at[0],
            recv_sem=frecv.at[late + i % turns],
            device_id={"sp": dest},
            device_id_type=MESH,
        )

    def send_near(k):
        return pltpu.make_async_remote_copy(
            src_ref=kvs.at[k],
            dst_ref=kvn.at[local],
            send_sem=sent.at[1],
            recv_sem=recv.at[0],
            device_id={"sp": near_to(k)},
            device_id_type=MESH,
        )

    def send_line(i):
        return pltpu.make_async_remote_copy(
            src_ref=kvs.at[half - 1 + i],
            dst_ref=kvf.at[local],
            send_sem=sent.at[1],
            recv_sem=recv.at[3],
            device_id={"sp": far_base + i * line + y},
            device_id_type=MESH,
        )

    def send_gates(k):
        dest = lax.rem(sp + k, n)
        return pltpu.make_async_remote_copy(
            src_ref=gsend.at[dest],
            dst_ref=grecv.at[sp],
            send_sem=sent.at[2],
            recv_sem=recv.at[1],
            device_id={"sp": dest},
            device_id_type=MESH,
        )

    def spread(j, k):
        piece = xfar.at[tp, far_from(k)]
        return pltpu.make_async_remote_copy(
            src_ref=piece,
            dst_ref=piece,
            send_sem=sent.at[3],
            recv_sem=xrecv.at[k],
            device_id={"tp": lax.rem(x + j, chips) * cores + c},
            device_id_type=MESH,
        )

    def hand(j, k):
        origin = lax.rem(x + chips - j, chips) * cores + c
        piece = xfar.at[origin, far_from(k)]
        return pltpu.make_async_remote_copy(
            src_ref=piece,
            dst_ref=piece,
            send_sem=sent.at[4],
            recv_sem=drecv.at[k // 2],
            device_id={"tp": partner},
            device_id_type=MESH,
        )

    def give(j):
        peer = lax.rem(tp + j, tpn)
        return pltpu.make_async_remote_copy(
            src_ref=parts.at[peer],
            dst_ref=got.at[j],
            send_sem=sent.at[5],
            recv_sem=recv.at[2],
            device_id={"tp": peer},
            device_id_type=MESH,
        )

    for copy in gate_loads:
        copy.start()
    for i in range(pieces):
        load(i).start()
    for copy in weight_loads + late_loads:
        copy.start()

    arrived(gate_w, lsem.at[4])
    wg[...] = jnp.concatenate(
        [gate_w[0].astype(F32), gate_w[1].astype(F32), jnp.zeros((wg.shape[0] - 4, depth), F32)],
        axis=0,
    ).astype(BF16)

    def rows_of(dest):
        return xall[pl.ds(dest * seqs, seqs)].reshape(rows, depth)

    def gates(start, stop):
        for i in range(start, stop):
            if i < half and i % (2 * half // pieces) == 0:
                load(i // (2 * half // pieces)).wait()
            dest = (near_base if i < half else far_base) + i % half
            gsend[pl.ds(dest, 1)] = nt(wg[...], rows_of(dest))[:4][None]

    gates(0, half)
    pl.semaphore_wait(barrier, n - 1 + tpn - 1)
    inner = jnp.logical_not(edge)
    for i in range(pieces // 2, pieces):
        load(i).wait()

    @pl.when(edge)
    def _():
        for i in range(steps):
            send_far(i).start()

    gates(half, 2 * half)
    grecv[pl.ds(sp, 1)] = gsend[pl.ds(sp, 1)]
    for k in range(1, n):
        send_gates(k).start()
    arrived(wkv, lsem.at[5])

    def keys_values(dest):
        return jnp.dot(rows_of(dest), wkv[...], preferred_element_type=F32).astype(BF16)

    for k in NEAR_ORDER:
        if k == "far":

            @pl.when(inner)
            def _():
                for i in range(steps):
                    send_far(i).start()

            continue
        kvs[k] = keys_values(near_to(k))
        send_near(k).start()
    for i in range(2):
        kvs[half - 1 + i] = keys_values(far_base + i * line + y)
        send_line(i).start()
    kvn[pl.ds(local, 1)] = keys_values(near_to(half - 1))[None]

    def weigh():
        lane = iota((rows, rows), 1)
        down = iota((rows, rows), 0)
        same = (lane // block) == (down // block)
        upto = (same & (down <= lane)).astype(F32)
        whole = same.astype(F32)
        before = (
            (iota((2 * n, 2 * n), 0) // n == iota((2 * n, 2 * n), 1) // n)
            & (iota((2 * n, 2 * n), 1) < iota((2 * n, 2 * n), 0))
        ).astype(F32)
        pre = [
            grecv[:, i, :] + biases[i // 2, 0:1, i % 2 : i % 2 + 1]
            for i in range(4)
        ]
        forget_pre = jnp.concatenate(pre[2:], axis=0)
        forget = jnp.minimum(forget_pre, 0.0) - jnp.log1p(jnp.exp(-jnp.abs(forget_pre)))
        inside = jnp.dot(forget, upto, preferred_element_type=F32, precision=HIGHEST)
        sums = jnp.dot(forget, whole, preferred_element_type=F32, precision=HIGHEST)
        running = jnp.dot(before, sums, preferred_element_type=F32, precision=HIGHEST) + inside
        totals = [jnp.sum(sums[g * n : (g + 1) * n], axis=0, keepdims=True) for g in range(2)]
        logs = [
            pre[0] + totals[0] - running[:n],
            pre[1] + running[n:] - forget[n:],
        ]
        peak = jnp.concatenate(
            [jnp.maximum(totals[g], jnp.max(logs[g], axis=0, keepdims=True)) for g in range(2)]
            + [jnp.zeros((6, rows), F32)],
            axis=0,
        )
        spot = iota(peak.shape, 1)
        step = 1
        while step < block:
            low, high = pltpu.roll(peak, step, 1), pltpu.roll(peak, rows - step, 1)
            peak = jnp.maximum(peak, jnp.where((spot & step) != 0, low, high))
            step *= 2
        weight = [jnp.exp(logs[g] - peak[g : g + 1]) * width ** (-0.5) for g in range(2)]
        first = side == 0
        parted = [jnp.where(first, w[:half], w[half:]) for w in weight]
        parted += [jnp.where(first, w[half:], w[:half]) for w in weight]
        cols[...] = jnp.concatenate(parted, axis=0).T
        own = iota((seqs, rows), 1) // block == iota((seqs, rows), 0)
        return [
            jnp.max(jnp.where(own, peak[g : g + 1], -jnp.inf), axis=1, keepdims=True)
            for g in range(2)
        ]

    def widen(i):
        for q in range(seqs):
            for s in range(half):
                j = i * half + s
                wb[i, q, s] = jnp.broadcast_to(
                    cols[q * block : (q + 1) * block, j : j + 1], (block, width)
                )

    def outer(kv, i, q):
        lines = slice(q * block, (q + 1) * block)
        keys = kv[:, lines, :width].reshape(half * block, width)
        values = kv[:, lines, width:].reshape(half * block, width).astype(F32)
        w0 = wb[2 * i, q].reshape(half * block, width)
        w1 = wb[2 * i + 1, q].reshape(half * block, width)
        weighted = jnp.concatenate([values * w0, values * w1], axis=1).astype(BF16)
        keys_f = keys.astype(F32)
        sums = [jnp.sum(keys_f * w, axis=0, keepdims=True) for w in (w0, w1)]
        return tn(keys, weighted), sums

    def project(p):
        found = [far_from(2 * p), far_from(2 * p + 1)]
        lines = [xfar[:, pl.ds(source, 1)].reshape(rows, depth) for source in found]
        both = jnp.dot(
            jnp.concatenate(lines, axis=0), wkv[...], preferred_element_type=F32
        ).astype(BF16)
        for i, source in enumerate(found):
            kvf[pl.ds(source, 1)] = both[i * rows : (i + 1) * rows][None]

    def own(k):
        arrived(xfar.at[0, 0], frecv.at[k])
        for j in (2, 1, 3):
            spread(j, k).start()
        hand(0, k).start()

    def pass_on(k):
        arrived(xfar.at[pl.ds(1, chips - 1), 0], xrecv.at[k])
        for j in (1, 3, 2):
            hand(j, k).start()

    def collect(p):
        arrived(xfar.at[pl.ds(0, chips), pl.ds(0, 2)], drecv.at[p])
        project(p)

    def queries():
        arrived(biases, lsem.at[6])
        for copy in late_loads[2:]:
            copy.wait()
        turned = query[...].astype(F32).T
        for q in range(seqs):
            qb[q] = jnp.broadcast_to(turned[:, q : q + 1], (width, width))

    stables = []

    def gates_in():
        arrived(grecv.at[pl.ds(0, n - 1)], recv.at[1])
        stables.extend(weigh())

    def widened(i):
        widen(i)

    def near_part():
        arrived(kvn.at[pl.ds(0, half - 1)], recv.at[0])
        for q in range(seqs):
            acc[q], sums = outer(kvn, 0, q)
            for g in range(2):
                nrm[g, q : q + 1] = sums[g]

    jobs = {
        "own": own, "pass": pass_on, "collect": collect, "widen": widened,
        "queries": lambda _: queries(), "gates": lambda _: gates_in(), "near": lambda _: near_part(),
    }
    for job, at in ORDER:
        jobs[job](at)
    arrived(kvf.at[pl.ds(0, 2)], recv.at[3])
    for q in range(seqs):
        more, sums = outer(kvf, 1, q)
        memory = (acc[q] + more).astype(BF16)
        back = memory.astype(F32)
        for g in range(2):
            membuf[g, q, 0] = memory[:, g * width : (g + 1) * width]
            num[g, q : q + 1] = jnp.sum(
                qb[q] * back[:, g * width : (g + 1) * width], axis=0, keepdims=True
            )
            total = nrm[g, q : q + 1] + sums[g]
            nrm[g, q : q + 1] = total
            norm_out[g, q] = total

    hidden = jnp.zeros((seqs, width), F32)
    queries = query[...].astype(F32)
    for g in range(2):
        under = jnp.abs(jnp.sum(queries * nrm[g], axis=1, keepdims=True))
        floor = jnp.maximum(jnp.exp(-stables[g]), 1.0)
        hidden = hidden + num[g] / jnp.maximum(under, floor)
        square = iota((seqs, width), 1) == iota((seqs, width), 0)
        row = jnp.sum(jnp.where(square, stables[g], 0.0), axis=0, keepdims=True)
        stab_out[g] = row[:, :seqs]
    terms = jnp.dot(hidden.astype(BF16), wo[...], preferred_element_type=F32)
    share = terms.shape[1] // tpn
    for t in range(tpn):
        parts[t] = terms[:, t * share : (t + 1) * share]
    for j in range(1, tpn):
        give(j).start()
    arrived(xfar.at[0, pl.ds(0, steps)], sent.at[0])
    arrived(kvs, sent.at[1])
    arrived(grecv.at[pl.ds(0, n - 1)], sent.at[2])
    arrived(xfar.at[pl.ds(0, chips - 1), pl.ds(0, steps)], sent.at[3])
    arrived(xfar.at[pl.ds(0, chips), pl.ds(0, steps)], sent.at[4])
    arrived(got.at[pl.ds(0, tpn - 1)], sent.at[5])
    arrived(got.at[pl.ds(0, tpn - 1)], recv.at[2])
    total = parts[tp]
    for j in range(1, tpn):
        total = total + got[j]
    read_out[...] = total.astype(BF16)


def publish(count, *refs):
    sources, targets, sems = refs[:count], refs[count : 2 * count], refs[2 * count]
    copies = [
        pltpu.make_async_copy(a, b, sems.at[i]) for i, (a, b) in enumerate(zip(sources, targets))
    ]
    for copy in copies:
        copy.start()
    for copy in copies:
        copy.wait()


def solution(mesh):
    n, tpn = mesh.shape["sp"], mesh.shape["tp"]

    def body(prompt, w_key, w_value, w_in_gate, w_forget_gate, in_bias, forget_bias, query, w_out):
        depth, heads, width = w_key.shape
        seqs = prompt.shape[0] // n
        block = prompt.shape[1]
        rows = seqs * block
        half = n // 2
        chips = tpn // 2
        steps = 2 * (half // 2 - 1)
        wo = w_out.reshape(heads * width, -1)
        columns = wo.shape[1]
        any_ = pl.BlockSpec(memory_space=pl.ANY)
        vmem = pl.BlockSpec(memory_space=pltpu.VMEM)
        dma = pltpu.SemaphoreType.DMA
        shapes = (
            ((2, seqs, heads, width, width), BF16),
            ((2, seqs, heads, width), F32),
            ((2, heads, seqs), F32),
            ((seqs, columns // tpn), BF16),
        )
        held = pl.pallas_call(
            functools.partial(kernel, n, tpn),
            out_shape=tuple(pltpu.VMEM(*shape) for shape in shapes),
            in_specs=[any_] * 9,
            out_specs=(vmem,) * 4,
            scratch_shapes=[
                pltpu.VMEM((n * seqs, block, depth), BF16),
                pltpu.VMEM((depth, 2 * width), BF16),
                pltpu.VMEM((width, columns), BF16),
                pltpu.VMEM((2, 2, depth), BF16),
                pltpu.VMEM((2, 1, 2), F32),
                pltpu.VMEM((seqs, width), BF16),
                pltpu.VMEM((16, depth), BF16),
                pltpu.VMEM((half + 1, rows, 2 * width), BF16),
                pltpu.VMEM((half, rows, 2 * width), BF16),
                pltpu.VMEM((half, rows, 2 * width), BF16),
                pltpu.VMEM((n, 4, rows), F32),
                pltpu.VMEM((n, 4, rows), F32),
                pltpu.VMEM((seqs, half, block, depth), BF16),
                pltpu.VMEM((rows, 4 * half), F32),
                pltpu.VMEM((4, seqs, half, block, width), F32),
                pltpu.VMEM((seqs, width, width), F32),
                pltpu.VMEM((seqs, width, 2 * width), F32),
                pltpu.VMEM((2, seqs, width), F32),
                pltpu.VMEM((2, seqs, width), F32),
                pltpu.VMEM((tpn, seqs, columns // tpn), F32),
                pltpu.VMEM((tpn, seqs, columns // tpn), F32),
                dma((9,)),
                dma((steps,)),
                dma((steps,)),
                dma((steps // 2,)),
                dma((4,)),
                dma((6,)),
            ],
            compiler_params=pltpu.CompilerParams(collective_id=0, has_side_effects=True),
            name="memories",
        )(
            prompt, w_key.reshape(depth, width), w_value.reshape(depth, width), wo,
            w_in_gate.reshape(2, depth), w_forget_gate.reshape(2, depth),
            in_bias.reshape(1, 2), forget_bias.reshape(1, 2), query.reshape(seqs, width),
        )
        memory, normal, stable, read = pl.pallas_call(
            functools.partial(publish, len(shapes)),
            out_shape=tuple(jax.ShapeDtypeStruct(*shape) for shape in shapes),
            in_specs=[vmem] * len(shapes),
            out_specs=(any_,) * len(shapes),
            scratch_shapes=[dma((len(shapes),))],
            name="outputs",
        )(*[pltpu.with_memory_space_constraint(a, pltpu.VMEM) for a in held])
        return memory, normal, stable.transpose(0, 2, 1), read

    return jax.shard_map(
        body,
        mesh=mesh,
        in_specs=(
            P("gr", "sp", None),
            P(None, "tp", None),
            P(None, "tp", None),
            P(None, None, "tp"),
            P(None, None, "tp"),
            P(None, "tp"),
            P(None, "tp"),
            P(("gr", "sp"), "tp", None),
            P("tp", None, None),
        ),
        out_specs=(
            P(None, ("gr", "sp"), "tp", None, None),
            P(None, ("gr", "sp"), "tp", None),
            P(None, ("gr", "sp"), "tp"),
            P(("gr", "sp"), "tp"),
        ),
        check_vma=False,
    )
```

```python
import functools

import jax
import jax.numpy as jnp
from jax import lax
from jax.experimental import pallas as pl
from jax.experimental.pallas import tpu as pltpu
from jax.sharding import PartitionSpec as P

MESH = pl.DeviceIdType.MESH
F32 = jnp.float32
BF16 = jnp.bfloat16
HIGHEST = lax.Precision.HIGHEST


def nt(a, b):
    return lax.dot_general(a, b, (((1,), (1,)), ((), ())), preferred_element_type=F32)


def tn(a, b):
    return lax.dot_general(a, b, (((0,), (0,)), ((), ())), preferred_element_type=F32)


def iota(shape, axis):
    return lax.broadcasted_iota(jnp.int32, shape, axis)


EDGE_TURNS = (0, 2, 1, 3)
RAW_TURNS = (2, 3)
LINE_TURNS = (0, 1)
FIRST = (
    ("gates", 0),
    ("gates", 1),
    ("barrier", 0),
    ("loaded", 0),
    ("edge", 0),
    ("gates", 2),
    ("gates", 3),
    ("send", 0),
    ("edge", 1),
    ("weights", 0),
    ("inner", 0),
    ("same", 0),
    ("other", 0),
    ("line", 0),
    ("own", 0),
)
ORDER = (
    ("own", 0),
    ("own", 1),
    ("queries", 0),
    ("own", 2),
    ("own", 3),
    ("pass", 0),
    ("own", 4),
    ("pass", 1),
    ("own", 5),
    ("pass", 2),
    ("gates", 0),
    ("pass", 3),
    ("widen", 0),
    ("widen", 1),
    ("widen", 2),
    ("pass", 4),
    ("widen", 3),
    ("collect", 0),
    ("pass", 5),
    ("collect", 1),
    ("near", 0),
    ("collect", 2),
)


def kernel(
    n, tpn,
    prompt, wk_hbm, wv_hbm, wo_hbm, ig_hbm, fg_hbm, ib_hbm, fb_hbm, q_hbm,
    membuf, norm_out, stab_out, read_out,
    xall, wkv, wo, gate_w, biases, query,
    wg, kvs, kvn, kvf, gsend, grecv, xfar, cols, wb, qb, acc, num, nrm, parts, got,
    lsem, frecv, xrecv, drecv, recv, sent,
):
    sp = lax.axis_index("sp")
    tp = lax.axis_index("tp")
    half = n // 2
    cores = 2
    chips = tpn // cores
    seqs, _, block, depth = xfar.shape
    rows = seqs * block
    width = wo.shape[0]
    line = half // 2
    side = sp // half
    local = sp - side * half
    deck, y = local // line, lax.rem(local, line)
    edge = deck == side
    near_base = side * half
    far_base = half - near_base
    x, c = tp // cores, lax.rem(tp, cores)
    partner = x * cores + 1 - c

    barrier = pltpu.get_barrier_semaphore()
    for i in range(half):
        pl.semaphore_signal(
            barrier,
            inc=1,
            device_id={"sp": far_base + lax.rem(local + half // 2 + i, half)},
            device_id_type=MESH,
        )
    for k in range(1, half):
        pl.semaphore_signal(
            barrier,
            inc=1,
            device_id={"sp": near_base + lax.rem(local + k, half)},
            device_id_type=MESH,
        )
    for j in range(1, tpn):
        pl.semaphore_signal(
            barrier, inc=1, device_id={"tp": lax.rem(tp + j, tpn)}, device_id_type=MESH
        )

    first, steps = len(EDGE_TURNS), len(EDGE_TURNS) + len(RAW_TURNS)

    def far_from(k):
        deck_of = 1 - side if k < first else side
        turn = (EDGE_TURNS + RAW_TURNS)[k]
        return deck_of * line + lax.rem(y + line - turn, line)

    def far_to(i, turns):
        deck_of = 1 - side if i < len(turns) else side
        return far_base + deck_of * line + lax.rem(y + turns[i % len(turns)], line)

    def near_to(deck_of, turn):
        return deck_of * line + lax.rem(y + turn, line)

    pieces = 4

    def load(i):
        base = (near_base if i < pieces // 2 else far_base) + i % (pieces // 2) * (2 * half // pieces)
        part = pl.ds(base * seqs, 2 * half // pieces * seqs)
        return pltpu.make_async_copy(prompt.at[part], xall.at[part], lsem.at[i])

    gate_loads = [
        pltpu.make_async_copy(ig_hbm, gate_w.at[0], lsem.at[4]),
        pltpu.make_async_copy(fg_hbm, gate_w.at[1], lsem.at[4]),
    ]
    weight_loads = [
        pltpu.make_async_copy(wk_hbm, wkv.at[:, :width], lsem.at[5]),
        pltpu.make_async_copy(wv_hbm, wkv.at[:, width:], lsem.at[5]),
    ]
    late_loads = [
        pltpu.make_async_copy(ib_hbm, biases.at[0], lsem.at[6]),
        pltpu.make_async_copy(fb_hbm, biases.at[1], lsem.at[6]),
        pltpu.make_async_copy(q_hbm, query, lsem.at[7]),
        pltpu.make_async_copy(wo_hbm, wo, lsem.at[8]),
    ]

    def arrived(ref, sem):
        pltpu.make_async_copy(ref, ref, sem).wait()

    def send_far(i, turns, base):
        dest = far_to(i, turns)
        return pltpu.make_async_remote_copy(
            src_ref=xall.at[dest * seqs + tp],
            dst_ref=xfar.at[tp, local],
            send_sem=sent.at[0],
            recv_sem=frecv.at[base + i % len(turns)],
            device_id={"sp": dest},
            device_id_type=MESH,
        )

    def far_from_edge(at):
        for i in range(at * first, (at + 1) * first):
            send_far(i, EDGE_TURNS, 0).start()

    def far_from_inner():
        for i in range(2 * len(RAW_TURNS)):
            send_far(i, RAW_TURNS, first).start()

    def send_near(deck_of, turn):
        dest = near_to(deck_of, turn)
        return pltpu.make_async_remote_copy(
            src_ref=kvs.at[dest],
            dst_ref=kvn.at[local],
            send_sem=sent.at[1],
            recv_sem=recv.at[0],
            device_id={"sp": near_base + dest},
            device_id_type=MESH,
        )

    def send_line(i):
        return pltpu.make_async_remote_copy(
            src_ref=kvs.at[half + i],
            dst_ref=kvf.at[local],
            send_sem=sent.at[6],
            recv_sem=recv.at[3],
            device_id={"sp": far_to(i, LINE_TURNS)},
            device_id_type=MESH,
        )

    def send_gates(k):
        dest = lax.rem(sp + k, n)
        return pltpu.make_async_remote_copy(
            src_ref=gsend.at[dest],
            dst_ref=grecv.at[sp],
            send_sem=sent.at[2],
            recv_sem=recv.at[1],
            device_id={"sp": dest},
            device_id_type=MESH,
        )

    def spread(j, k):
        piece = xfar.at[tp, far_from(k)]
        return pltpu.make_async_remote_copy(
            src_ref=piece,
            dst_ref=piece,
            send_sem=sent.at[3],
            recv_sem=xrecv.at[k],
            device_id={"tp": lax.rem(x + j, chips) * cores + c},
            device_id_type=MESH,
        )

    def hand(j, k):
        origin = lax.rem(x + chips - j, chips) * cores + c
        piece = xfar.at[origin, far_from(k)]
        return pltpu.make_async_remote_copy(
            src_ref=piece,
            dst_ref=piece,
            send_sem=sent.at[4],
            recv_sem=drecv.at[k // 2],
            device_id={"tp": partner},
            device_id_type=MESH,
        )

    def give(j):
        peer = lax.rem(tp + j, tpn)
        return pltpu.make_async_remote_copy(
            src_ref=parts.at[peer],
            dst_ref=got.at[j],
            send_sem=sent.at[5],
            recv_sem=recv.at[2],
            device_id={"tp": peer},
            device_id_type=MESH,
        )

    for copy in gate_loads:
        copy.start()
    for i in range(pieces):
        load(i).start()
    for copy in weight_loads + late_loads:
        copy.start()

    arrived(gate_w, lsem.at[4])
    wg[...] = jnp.concatenate(
        [gate_w[0].astype(F32), gate_w[1].astype(F32), jnp.zeros((wg.shape[0] - 4, depth), F32)],
        axis=0,
    ).astype(BF16)

    def rows_of(dest):
        return xall[pl.ds(dest * seqs, seqs)].reshape(rows, depth)

    def gates(start, stop):
        for i in range(start, stop):
            if i < half and i % (2 * half // pieces) == 0:
                load(i // (2 * half // pieces)).wait()
            dest = (near_base if i < half else far_base) + i % half
            gsend[pl.ds(dest, 1)] = nt(wg[...], rows_of(dest))[:4][None]

    inner = jnp.logical_not(edge)

    def start_gates():
        grecv[pl.ds(sp, 1)] = gsend[pl.ds(sp, 1)]
        for k in range(1, n):
            send_gates(k).start()

    def keys_values(blocks, base):
        lines = [rows_of(dest) for dest in blocks]
        both = jnp.dot(
            jnp.concatenate(lines, axis=0), wkv[...], preferred_element_type=F32
        ).astype(BF16)
        kvs[pl.ds(base, len(blocks))] = both.reshape(len(blocks), rows, 2 * width)

    def near_other():
        base = (1 - deck) * line
        keys_values([near_base + base + i for i in range(line)], base)
        for turn in (2, 1, 3, 0):
            send_near(1 - deck, turn).start()

    def near_same():
        base = deck * line
        keys_values([near_base + base + i for i in range(line)], base)
        for turn in (2, 1, 3):
            send_near(deck, turn).start()

    def own_near():
        kvn[pl.ds(local, 1)] = kvs[pl.ds(local, 1)]

    def lines():
        count = 2 * len(LINE_TURNS)
        keys_values([far_to(i, LINE_TURNS) for i in range(count)], half)
        for i in range(count):
            send_line(i).start()

    first_jobs = {
        "barrier": lambda _: pl.semaphore_wait(barrier, n - 1 + tpn - 1),
        "loaded": lambda _: [load(i).wait() for i in range(pieces // 2, pieces)],
        "edge": lambda at: pl.when(edge)(functools.partial(far_from_edge, at)),
        "inner": lambda _: pl.when(inner)(far_from_inner),
        "gates": lambda at: gates(at * half // 2, (at + 1) * half // 2),
        "send": lambda _: start_gates(),
        "weights": lambda _: arrived(wkv, lsem.at[5]),
        "other": lambda _: near_other(),
        "same": lambda _: near_same(),
        "own": lambda _: own_near(),
        "line": lambda _: pl.when(inner)(lines),
    }
    for job, at in FIRST:
        first_jobs[job](at)

    def weigh():
        lane = iota((rows, rows), 1)
        down = iota((rows, rows), 0)
        same = (lane // block) == (down // block)
        upto = (same & (down <= lane)).astype(F32)
        whole = same.astype(F32)
        before = (
            (iota((2 * n, 2 * n), 0) // n == iota((2 * n, 2 * n), 1) // n)
            & (iota((2 * n, 2 * n), 1) < iota((2 * n, 2 * n), 0))
        ).astype(F32)
        pre = [
            grecv[:, i, :] + biases[i // 2, 0:1, i % 2 : i % 2 + 1]
            for i in range(4)
        ]
        forget_pre = jnp.concatenate(pre[2:], axis=0)
        forget = jnp.minimum(forget_pre, 0.0) - jnp.log1p(jnp.exp(-jnp.abs(forget_pre)))
        inside = jnp.dot(forget, upto, preferred_element_type=F32, precision=HIGHEST)
        sums = jnp.dot(forget, whole, preferred_element_type=F32, precision=HIGHEST)
        running = jnp.dot(before, sums, preferred_element_type=F32, precision=HIGHEST) + inside
        totals = [jnp.sum(sums[g * n : (g + 1) * n], axis=0, keepdims=True) for g in range(2)]
        logs = [
            pre[0] + totals[0] - running[:n],
            pre[1] + running[n:] - forget[n:],
        ]
        peak = jnp.concatenate(
            [jnp.maximum(totals[g], jnp.max(logs[g], axis=0, keepdims=True)) for g in range(2)]
            + [jnp.zeros((6, rows), F32)],
            axis=0,
        )
        spot = iota(peak.shape, 1)
        step = 1
        while step < block:
            low, high = pltpu.roll(peak, step, 1), pltpu.roll(peak, rows - step, 1)
            peak = jnp.maximum(peak, jnp.where((spot & step) != 0, low, high))
            step *= 2
        weight = [jnp.exp(logs[g] - peak[g : g + 1]) * width ** (-0.5) for g in range(2)]
        first = side == 0
        parted = [jnp.where(first, w[:half], w[half:]) for w in weight]
        parted += [jnp.where(first, w[half:], w[:half]) for w in weight]
        cols[...] = jnp.concatenate(parted, axis=0).T
        own = iota((seqs, rows), 1) // block == iota((seqs, rows), 0)
        return [
            jnp.max(jnp.where(own, peak[g : g + 1], -jnp.inf), axis=1, keepdims=True)
            for g in range(2)
        ]

    def widen(i):
        for q in range(seqs):
            for s in range(half):
                j = i * half + s
                wb[i, q, s] = jnp.broadcast_to(
                    cols[q * block : (q + 1) * block, j : j + 1], (block, width)
                )

    def outer(kv, i, q):
        lines = slice(q * block, (q + 1) * block)
        keys = kv[:, lines, :width].reshape(half * block, width)
        values = kv[:, lines, width:].reshape(half * block, width).astype(F32)
        w0 = wb[2 * i, q].reshape(half * block, width)
        w1 = wb[2 * i + 1, q].reshape(half * block, width)
        weighted = jnp.concatenate([values * w0, values * w1], axis=1).astype(BF16)
        keys_f = keys.astype(F32)
        sums = [jnp.sum(keys_f * w, axis=0, keepdims=True) for w in (w0, w1)]
        return tn(keys, weighted), sums

    def project(p):
        found = [far_from(2 * p), far_from(2 * p + 1)]
        lines = [xfar[:, pl.ds(source, 1)].reshape(rows, depth) for source in found]
        both = jnp.dot(
            jnp.concatenate(lines, axis=0), wkv[...], preferred_element_type=F32
        ).astype(BF16)
        for i, source in enumerate(found):
            kvf[pl.ds(source, 1)] = both[i * rows : (i + 1) * rows][None]

    def own(k):
        arrived(xfar.at[0, 0], frecv.at[k])
        for j in (2, 1, 3):
            spread(j, k).start()
        hand(0, k).start()

    def pass_on(k):
        arrived(xfar.at[pl.ds(1, chips - 1), 0], xrecv.at[k])
        for j in (1, 3, 2):
            hand(j, k).start()

    def collect(p):
        arrived(xfar.at[pl.ds(0, chips), pl.ds(0, 2)], drecv.at[p])
        project(p)

    def queries():
        arrived(biases, lsem.at[6])
        for copy in late_loads[2:]:
            copy.wait()
        turned = query[...].astype(F32).T
        for q in range(seqs):
            qb[q] = jnp.broadcast_to(turned[:, q : q + 1], (width, width))

    stables = []

    def gates_in():
        arrived(grecv.at[pl.ds(0, n - 1)], recv.at[1])
        stables.extend(weigh())

    def widened(i):
        widen(i)

    def near_part():
        arrived(kvn.at[pl.ds(0, half - 1)], recv.at[0])
        for q in range(seqs):
            acc[q], sums = outer(kvn, 0, q)
            for g in range(2):
                nrm[g, q : q + 1] = sums[g]

    jobs = {
        "own": own, "pass": pass_on, "collect": collect, "widen": widened,
        "queries": lambda _: queries(), "gates": lambda _: gates_in(), "near": lambda _: near_part(),
    }
    for job, at in ORDER:
        jobs[job](at)
    arrived(kvf.at[pl.ds(0, len(LINE_TURNS))], recv.at[3])
    for q in range(seqs):
        more, sums = outer(kvf, 1, q)
        memory = (acc[q] + more).astype(BF16)
        back = memory.astype(F32)
        for g in range(2):
            membuf[g, q, 0] = memory[:, g * width : (g + 1) * width]
            num[g, q : q + 1] = jnp.sum(
                qb[q] * back[:, g * width : (g + 1) * width], axis=0, keepdims=True
            )
            total = nrm[g, q : q + 1] + sums[g]
            nrm[g, q : q + 1] = total
            norm_out[g, q] = total

    hidden = jnp.zeros((seqs, width), F32)
    queries = query[...].astype(F32)
    for g in range(2):
        under = jnp.abs(jnp.sum(queries * nrm[g], axis=1, keepdims=True))
        floor = jnp.maximum(jnp.exp(-stables[g]), 1.0)
        hidden = hidden + num[g] / jnp.maximum(under, floor)
        square = iota((seqs, width), 1) == iota((seqs, width), 0)
        row = jnp.sum(jnp.where(square, stables[g], 0.0), axis=0, keepdims=True)
        stab_out[g] = row[:, :seqs]
    terms = jnp.dot(hidden.astype(BF16), wo[...], preferred_element_type=F32)
    share = terms.shape[1] // tpn
    for t in range(tpn):
        parts[t] = terms[:, t * share : (t + 1) * share]
    for j in range(1, tpn):
        give(j).start()
    @pl.when(edge)
    def _():
        arrived(xfar.at[0, pl.ds(0, 2 * first)], sent.at[0])

    @pl.when(inner)
    def _():
        arrived(xfar.at[0, pl.ds(0, 2 * len(RAW_TURNS))], sent.at[0])
        arrived(kvs.at[pl.ds(0, 2 * len(LINE_TURNS))], sent.at[6])

    arrived(kvs.at[pl.ds(0, half - 1)], sent.at[1])
    arrived(grecv.at[pl.ds(0, n - 1)], sent.at[2])
    arrived(xfar.at[pl.ds(0, chips - 1), pl.ds(0, steps)], sent.at[3])
    arrived(xfar.at[pl.ds(0, chips), pl.ds(0, steps)], sent.at[4])
    arrived(got.at[pl.ds(0, tpn - 1)], sent.at[5])
    arrived(got.at[pl.ds(0, tpn - 1)], recv.at[2])
    total = parts[tp]
    for j in range(1, tpn):
        total = total + got[j]
    read_out[...] = total.astype(BF16)


def publish(count, *refs):
    sources, targets, sems = refs[:count], refs[count : 2 * count], refs[2 * count]
    copies = [
        pltpu.make_async_copy(a, b, sems.at[i]) for i, (a, b) in enumerate(zip(sources, targets))
    ]
    for copy in copies:
        copy.start()
    for copy in copies:
        copy.wait()


def solution(mesh):
    n, tpn = mesh.shape["sp"], mesh.shape["tp"]

    def body(prompt, w_key, w_value, w_in_gate, w_forget_gate, in_bias, forget_bias, query, w_out):
        depth, heads, width = w_key.shape
        seqs = prompt.shape[0] // n
        block = prompt.shape[1]
        rows = seqs * block
        half = n // 2
        chips = tpn // 2
        steps = len(EDGE_TURNS) + len(RAW_TURNS)
        wo = w_out.reshape(heads * width, -1)
        columns = wo.shape[1]
        any_ = pl.BlockSpec(memory_space=pl.ANY)
        vmem = pl.BlockSpec(memory_space=pltpu.VMEM)
        dma = pltpu.SemaphoreType.DMA
        shapes = (
            ((2, seqs, heads, width, width), BF16),
            ((2, seqs, heads, width), F32),
            ((2, heads, seqs), F32),
            ((seqs, columns // tpn), BF16),
        )
        held = pl.pallas_call(
            functools.partial(kernel, n, tpn),
            out_shape=tuple(pltpu.VMEM(*shape) for shape in shapes),
            in_specs=[any_] * 9,
            out_specs=(vmem,) * 4,
            scratch_shapes=[
                pltpu.VMEM((n * seqs, block, depth), BF16),
                pltpu.VMEM((depth, 2 * width), BF16),
                pltpu.VMEM((width, columns), BF16),
                pltpu.VMEM((2, 2, depth), BF16),
                pltpu.VMEM((2, 1, 2), F32),
                pltpu.VMEM((seqs, width), BF16),
                pltpu.VMEM((16, depth), BF16),
                pltpu.VMEM((half + 2 * len(LINE_TURNS), rows, 2 * width), BF16),
                pltpu.VMEM((half, rows, 2 * width), BF16),
                pltpu.VMEM((half, rows, 2 * width), BF16),
                pltpu.VMEM((n, 4, rows), F32),
                pltpu.VMEM((n, 4, rows), F32),
                pltpu.VMEM((seqs, half, block, depth), BF16),
                pltpu.VMEM((rows, 4 * half), F32),
                pltpu.VMEM((4, seqs, half, block, width), F32),
                pltpu.VMEM((seqs, width, width), F32),
                pltpu.VMEM((seqs, width, 2 * width), F32),
                pltpu.VMEM((2, seqs, width), F32),
                pltpu.VMEM((2, seqs, width), F32),
                pltpu.VMEM((tpn, seqs, columns // tpn), F32),
                pltpu.VMEM((tpn, seqs, columns // tpn), F32),
                dma((9,)),
                dma((steps,)),
                dma((steps,)),
                dma((steps // 2,)),
                dma((4,)),
                dma((7,)),
            ],
            compiler_params=pltpu.CompilerParams(collective_id=0, has_side_effects=True),
            name="memories",
        )(
            prompt, w_key.reshape(depth, width), w_value.reshape(depth, width), wo,
            w_in_gate.reshape(2, depth), w_forget_gate.reshape(2, depth),
            in_bias.reshape(1, 2), forget_bias.reshape(1, 2), query.reshape(seqs, width),
        )
        memory, normal, stable, read = pl.pallas_call(
            functools.partial(publish, len(shapes)),
            out_shape=tuple(jax.ShapeDtypeStruct(*shape) for shape in shapes),
            in_specs=[vmem] * len(shapes),
            out_specs=(any_,) * len(shapes),
            scratch_shapes=[dma((len(shapes),))],
            name="outputs",
        )(*[pltpu.with_memory_space_constraint(a, pltpu.VMEM) for a in held])
        return memory, normal, stable.transpose(0, 2, 1), read

    return jax.shard_map(
        body,
        mesh=mesh,
        in_specs=(
            P("gr", "sp", None),
            P(None, "tp", None),
            P(None, "tp", None),
            P(None, None, "tp"),
            P(None, None, "tp"),
            P(None, "tp"),
            P(None, "tp"),
            P(("gr", "sp"), "tp", None),
            P("tp", None, None),
        ),
        out_specs=(
            P(None, ("gr", "sp"), "tp", None, None),
            P(None, ("gr", "sp"), "tp", None),
            P(None, ("gr", "sp"), "tp"),
            P(("gr", "sp"), "tp"),
        ),
        check_vma=False,
    )
```

```python
import functools

import jax
import jax.numpy as jnp
from jax import lax
from jax.experimental import pallas as pl
from jax.experimental.pallas import tpu as pltpu
from jax.sharding import PartitionSpec as P

MESH = pl.DeviceIdType.MESH
F32 = jnp.float32
BF16 = jnp.bfloat16
HIGHEST = lax.Precision.HIGHEST


def nt(a, b):
    return lax.dot_general(a, b, (((1,), (1,)), ((), ())), preferred_element_type=F32)


def tn(a, b):
    return lax.dot_general(a, b, (((0,), (0,)), ((), ())), preferred_element_type=F32)


def iota(shape, axis):
    return lax.broadcasted_iota(jnp.int32, shape, axis)


EDGE_TURNS = (0, 2, 1, 3)
RAW_TO_END, RAW_TO_MIDDLE = (2, 3), (2,)
LINE_TO_END, LINE_TO_MIDDLE = (0, 1), (0, 1, 3)
GROUPS = ((0, 1), (2, 3), (4,), (5,))
FIRST = (
    ("gates", 0),
    ("gates", 1),
    ("barrier", 0),
    ("loaded", 0),
    ("edge", 0),
    ("edge", 1),
    ("inner", 0),
    ("gates", 2),
    ("gates", 3),
    ("send", 0),
    ("weights", 0),
    ("line", 0),
    ("same", 0),
    ("other", 0),
    ("own", 0),
)
ORDER = (
    ("own", 0),
    ("own", 1),
    ("queries", 0),
    ("own", 2),
    ("own", 3),
    ("pass", 0),
    ("own", 4),
    ("pass", 1),
    ("own", 5),
    ("pass", 2),
    ("gates", 0),
    ("pass", 3),
    ("widen", 0),
    ("widen", 1),
    ("widen", 2),
    ("pass", 4),
    ("widen", 3),
    ("collect", 0),
    ("pass", 5),
    ("collect", 1),
    ("collect", 2),
    ("collect", 3),
    ("near", 0),
)


def kernel(
    n, tpn,
    prompt, wk_hbm, wv_hbm, wo_hbm, ig_hbm, fg_hbm, ib_hbm, fb_hbm, q_hbm,
    membuf, norm_out, stab_out, read_out,
    xall, wkv, wo, gate_w, biases, query,
    wg, kvs, kvn, kvf, gsend, grecv, xfar, cols, wb, qb, acc, num, nrm, parts, got,
    lsem, frecv, xrecv, drecv, recv, sent,
):
    sp = lax.axis_index("sp")
    tp = lax.axis_index("tp")
    half = n // 2
    cores = 2
    chips = tpn // cores
    seqs, _, block, depth = xfar.shape
    rows = seqs * block
    width = wo.shape[0]
    line = half // 2
    side = sp // half
    local = sp - side * half
    deck, y = local // line, lax.rem(local, line)
    edge = deck == side
    near_base = side * half
    far_base = half - near_base
    x, c = tp // cores, lax.rem(tp, cores)
    partner = x * cores + 1 - c

    barrier = pltpu.get_barrier_semaphore()
    for i in range(half):
        pl.semaphore_signal(
            barrier,
            inc=1,
            device_id={"sp": far_base + lax.rem(local + half // 2 + i, half)},
            device_id_type=MESH,
        )
    for k in range(1, half):
        pl.semaphore_signal(
            barrier,
            inc=1,
            device_id={"sp": near_base + lax.rem(local + k, half)},
            device_id_type=MESH,
        )
    for j in range(1, tpn):
        pl.semaphore_signal(
            barrier, inc=1, device_id={"tp": lax.rem(tp + j, tpn)}, device_id_type=MESH
        )

    first = len(EDGE_TURNS)
    steps, shared = first + len(RAW_TO_END), first + len(RAW_TO_MIDDLE)

    def far_from(k):
        deck_of = 1 - side if k < first else side
        turn = (EDGE_TURNS + RAW_TO_END)[k]
        return deck_of * line + lax.rem(y + line - turn, line)

    def far_to(near_middle, turn):
        deck_of = side if near_middle else 1 - side
        return far_base + deck_of * line + lax.rem(y + turn, line)

    raw_to = [(False, turn) for turn in RAW_TO_END] + [(True, turn) for turn in RAW_TO_MIDDLE]
    line_to = [(False, turn) for turn in LINE_TO_END] + [(True, turn) for turn in LINE_TO_MIDDLE]

    def near_to(deck_of, turn):
        return deck_of * line + lax.rem(y + turn, line)

    pieces = 4

    def load(i):
        base = (near_base if i < pieces // 2 else far_base) + i % (pieces // 2) * (2 * half // pieces)
        part = pl.ds(base * seqs, 2 * half // pieces * seqs)
        return pltpu.make_async_copy(prompt.at[part], xall.at[part], lsem.at[i])

    gate_loads = [
        pltpu.make_async_copy(ig_hbm, gate_w.at[0], lsem.at[4]),
        pltpu.make_async_copy(fg_hbm, gate_w.at[1], lsem.at[4]),
    ]
    weight_loads = [
        pltpu.make_async_copy(wk_hbm, wkv.at[:, :width], lsem.at[5]),
        pltpu.make_async_copy(wv_hbm, wkv.at[:, width:], lsem.at[5]),
    ]
    late_loads = [
        pltpu.make_async_copy(ib_hbm, biases.at[0], lsem.at[6]),
        pltpu.make_async_copy(fb_hbm, biases.at[1], lsem.at[6]),
        pltpu.make_async_copy(q_hbm, query, lsem.at[7]),
        pltpu.make_async_copy(wo_hbm, wo, lsem.at[8]),
    ]

    def arrived(ref, sem):
        pltpu.make_async_copy(ref, ref, sem).wait()

    def send_far(near_middle, turn, slot):
        dest = far_to(near_middle, turn)
        return pltpu.make_async_remote_copy(
            src_ref=xall.at[dest * seqs + tp],
            dst_ref=xfar.at[tp, local],
            send_sem=sent.at[0],
            recv_sem=frecv.at[slot],
            device_id={"sp": dest},
            device_id_type=MESH,
        )

    def far_from_edge(at):
        for slot, turn in enumerate(EDGE_TURNS):
            send_far(at == 1, turn, slot).start()

    def far_from_inner():
        for i, (near_middle, turn) in enumerate(raw_to):
            send_far(near_middle, turn, first + i % len(RAW_TO_END)).start()

    def send_near(deck_of, turn):
        dest = near_to(deck_of, turn)
        return pltpu.make_async_remote_copy(
            src_ref=kvs.at[dest],
            dst_ref=kvn.at[local],
            send_sem=sent.at[1],
            recv_sem=recv.at[0],
            device_id={"sp": near_base + dest},
            device_id_type=MESH,
        )

    def send_line(i):
        return pltpu.make_async_remote_copy(
            src_ref=kvs.at[half + i],
            dst_ref=kvf.at[local],
            send_sem=sent.at[6],
            recv_sem=recv.at[3],
            device_id={"sp": far_to(*line_to[i])},
            device_id_type=MESH,
        )

    def send_gates(k):
        dest = lax.rem(sp + k, n)
        return pltpu.make_async_remote_copy(
            src_ref=gsend.at[dest],
            dst_ref=grecv.at[sp],
            send_sem=sent.at[2],
            recv_sem=recv.at[1],
            device_id={"sp": dest},
            device_id_type=MESH,
        )

    def spread(j, k):
        piece = xfar.at[tp, far_from(k)]
        return pltpu.make_async_remote_copy(
            src_ref=piece,
            dst_ref=piece,
            send_sem=sent.at[3],
            recv_sem=xrecv.at[k],
            device_id={"tp": lax.rem(x + j, chips) * cores + c},
            device_id_type=MESH,
        )

    def group_of(k):
        return [p for p, group in enumerate(GROUPS) if k in group][0]

    def hand(j, k):
        origin = lax.rem(x + chips - j, chips) * cores + c
        piece = xfar.at[origin, far_from(k)]
        return pltpu.make_async_remote_copy(
            src_ref=piece,
            dst_ref=piece,
            send_sem=sent.at[4],
            recv_sem=drecv.at[group_of(k)],
            device_id={"tp": partner},
            device_id_type=MESH,
        )

    def give(j):
        peer = lax.rem(tp + j, tpn)
        return pltpu.make_async_remote_copy(
            src_ref=parts.at[peer],
            dst_ref=got.at[j],
            send_sem=sent.at[5],
            recv_sem=recv.at[2],
            device_id={"tp": peer},
            device_id_type=MESH,
        )

    for copy in gate_loads:
        copy.start()
    for i in range(pieces):
        load(i).start()
    for copy in weight_loads + late_loads:
        copy.start()

    arrived(gate_w, lsem.at[4])
    wg[...] = jnp.concatenate(
        [gate_w[0].astype(F32), gate_w[1].astype(F32), jnp.zeros((wg.shape[0] - 4, depth), F32)],
        axis=0,
    ).astype(BF16)

    def rows_of(dest):
        return xall[pl.ds(dest * seqs, seqs)].reshape(rows, depth)

    def gates(start, stop):
        for i in range(start, stop):
            if i < half and i % (2 * half // pieces) == 0:
                load(i // (2 * half // pieces)).wait()
            dest = (near_base if i < half else far_base) + i % half
            gsend[pl.ds(dest, 1)] = nt(wg[...], rows_of(dest))[:4][None]

    inner = jnp.logical_not(edge)

    def start_gates():
        grecv[pl.ds(sp, 1)] = gsend[pl.ds(sp, 1)]
        for k in range(1, n):
            send_gates(k).start()

    def keys_values(blocks, base):
        lines = [rows_of(dest) for dest in blocks]
        both = jnp.dot(
            jnp.concatenate(lines, axis=0), wkv[...], preferred_element_type=F32
        ).astype(BF16)
        kvs[pl.ds(base, len(blocks))] = both.reshape(len(blocks), rows, 2 * width)

    def near_other():
        base = (1 - deck) * line
        keys_values([near_base + base + i for i in range(line)], base)
        for turn in (2, 1, 3, 0):
            send_near(1 - deck, turn).start()

    def near_same():
        base = deck * line
        keys_values([near_base + base + i for i in range(line)], base)
        for turn in (2, 1, 3):
            send_near(deck, turn).start()

    def own_near():
        kvn[pl.ds(local, 1)] = kvs[pl.ds(local, 1)]

    def lines():
        count = len(line_to)
        keys_values([far_to(*to) for to in line_to], half)
        for i in range(count):
            send_line(i).start()

    first_jobs = {
        "barrier": lambda _: pl.semaphore_wait(barrier, n - 1 + tpn - 1),
        "loaded": lambda _: [load(i).wait() for i in range(pieces // 2, pieces)],
        "edge": lambda at: pl.when(edge)(functools.partial(far_from_edge, at)),
        "inner": lambda _: pl.when(inner)(far_from_inner),
        "gates": lambda at: gates(at * half // 2, (at + 1) * half // 2),
        "send": lambda _: start_gates(),
        "weights": lambda _: arrived(wkv, lsem.at[5]),
        "other": lambda _: near_other(),
        "same": lambda _: near_same(),
        "own": lambda _: own_near(),
        "line": lambda _: pl.when(inner)(lines),
    }
    for job, at in FIRST:
        first_jobs[job](at)

    def weigh():
        lane = iota((rows, rows), 1)
        down = iota((rows, rows), 0)
        same = (lane // block) == (down // block)
        upto = (same & (down <= lane)).astype(F32)
        whole = same.astype(F32)
        before = (
            (iota((2 * n, 2 * n), 0) // n == iota((2 * n, 2 * n), 1) // n)
            & (iota((2 * n, 2 * n), 1) < iota((2 * n, 2 * n), 0))
        ).astype(F32)
        pre = [
            grecv[:, i, :] + biases[i // 2, 0:1, i % 2 : i % 2 + 1]
            for i in range(4)
        ]
        forget_pre = jnp.concatenate(pre[2:], axis=0)
        forget = jnp.minimum(forget_pre, 0.0) - jnp.log1p(jnp.exp(-jnp.abs(forget_pre)))
        inside = jnp.dot(forget, upto, preferred_element_type=F32, precision=HIGHEST)
        sums = jnp.dot(forget, whole, preferred_element_type=F32, precision=HIGHEST)
        running = jnp.dot(before, sums, preferred_element_type=F32, precision=HIGHEST) + inside
        totals = [jnp.sum(sums[g * n : (g + 1) * n], axis=0, keepdims=True) for g in range(2)]
        logs = [
            pre[0] + totals[0] - running[:n],
            pre[1] + running[n:] - forget[n:],
        ]
        peak = jnp.concatenate(
            [jnp.maximum(totals[g], jnp.max(logs[g], axis=0, keepdims=True)) for g in range(2)]
            + [jnp.zeros((6, rows), F32)],
            axis=0,
        )
        spot = iota(peak.shape, 1)
        step = 1
        while step < block:
            low, high = pltpu.roll(peak, step, 1), pltpu.roll(peak, rows - step, 1)
            peak = jnp.maximum(peak, jnp.where((spot & step) != 0, low, high))
            step *= 2
        weight = [jnp.exp(logs[g] - peak[g : g + 1]) * width ** (-0.5) for g in range(2)]
        first = side == 0
        parted = [jnp.where(first, w[:half], w[half:]) for w in weight]
        parted += [jnp.where(first, w[half:], w[:half]) for w in weight]
        cols[...] = jnp.concatenate(parted, axis=0).T
        own = iota((seqs, rows), 1) // block == iota((seqs, rows), 0)
        return [
            jnp.max(jnp.where(own, peak[g : g + 1], -jnp.inf), axis=1, keepdims=True)
            for g in range(2)
        ]

    def widen(i):
        for q in range(seqs):
            for s in range(half):
                j = i * half + s
                wb[i, q, s] = jnp.broadcast_to(
                    cols[q * block : (q + 1) * block, j : j + 1], (block, width)
                )

    def outer(kv, i, q):
        lines = slice(q * block, (q + 1) * block)
        keys = kv[:, lines, :width].reshape(half * block, width)
        values = kv[:, lines, width:].reshape(half * block, width).astype(F32)
        w0 = wb[2 * i, q].reshape(half * block, width)
        w1 = wb[2 * i + 1, q].reshape(half * block, width)
        weighted = jnp.concatenate([values * w0, values * w1], axis=1).astype(BF16)
        keys_f = keys.astype(F32)
        sums = [jnp.sum(keys_f * w, axis=0, keepdims=True) for w in (w0, w1)]
        return tn(keys, weighted), sums

    def project(p):
        found = [far_from(k) for k in GROUPS[p]]
        lines = [xfar[:, pl.ds(source, 1)].reshape(rows, depth) for source in found]
        both = jnp.dot(
            jnp.concatenate(lines, axis=0), wkv[...], preferred_element_type=F32
        ).astype(BF16)
        for i, source in enumerate(found):
            kvf[pl.ds(source, 1)] = both[i * rows : (i + 1) * rows][None]

    def own(k):
        arrived(xfar.at[0, 0], frecv.at[k])
        for j in (2, 1, 3):
            spread(j, k).start()
        hand(0, k).start()

    def pass_on(k):
        arrived(xfar.at[pl.ds(1, chips - 1), 0], xrecv.at[k])
        for j in (1, 3, 2):
            hand(j, k).start()

    def collect(p):
        arrived(xfar.at[pl.ds(0, chips), pl.ds(0, len(GROUPS[p]))], drecv.at[p])
        project(p)

    def queries():
        arrived(biases, lsem.at[6])
        for copy in late_loads[2:]:
            copy.wait()
        turned = query[...].astype(F32).T
        for q in range(seqs):
            qb[q] = jnp.broadcast_to(turned[:, q : q + 1], (width, width))

    stables = []

    def gates_in():
        arrived(grecv.at[pl.ds(0, n - 1)], recv.at[1])
        stables.extend(weigh())

    def widened(i):
        widen(i)

    def near_part():
        arrived(kvn.at[pl.ds(0, half - 1)], recv.at[0])
        for q in range(seqs):
            acc[q], sums = outer(kvn, 0, q)
            for g in range(2):
                nrm[g, q : q + 1] = sums[g]

    jobs = {
        "own": own, "pass": pass_on, "collect": collect, "widen": widened,
        "queries": lambda _: queries(), "gates": lambda _: gates_in(), "near": lambda _: near_part(),
    }
    for job, at in ORDER:
        slot = GROUPS[at][0] if job == "collect" else at if job in ("own", "pass") else 0
        if slot < shared:
            jobs[job](at)
        else:
            pl.when(edge)(functools.partial(jobs[job], at))
    @pl.when(edge)
    def _():
        arrived(kvf.at[pl.ds(0, len(LINE_TO_END))], recv.at[3])

    @pl.when(inner)
    def _():
        arrived(kvf.at[pl.ds(0, len(LINE_TO_MIDDLE))], recv.at[3])

    for q in range(seqs):
        more, sums = outer(kvf, 1, q)
        memory = (acc[q] + more).astype(BF16)
        back = memory.astype(F32)
        for g in range(2):
            membuf[g, q, 0] = memory[:, g * width : (g + 1) * width]
            num[g, q : q + 1] = jnp.sum(
                qb[q] * back[:, g * width : (g + 1) * width], axis=0, keepdims=True
            )
            total = nrm[g, q : q + 1] + sums[g]
            nrm[g, q : q + 1] = total
            norm_out[g, q] = total

    hidden = jnp.zeros((seqs, width), F32)
    queries = query[...].astype(F32)
    for g in range(2):
        under = jnp.abs(jnp.sum(queries * nrm[g], axis=1, keepdims=True))
        floor = jnp.maximum(jnp.exp(-stables[g]), 1.0)
        hidden = hidden + num[g] / jnp.maximum(under, floor)
        square = iota((seqs, width), 1) == iota((seqs, width), 0)
        row = jnp.sum(jnp.where(square, stables[g], 0.0), axis=0, keepdims=True)
        stab_out[g] = row[:, :seqs]
    terms = jnp.dot(hidden.astype(BF16), wo[...], preferred_element_type=F32)
    share = terms.shape[1] // tpn
    for t in range(tpn):
        parts[t] = terms[:, t * share : (t + 1) * share]
    for j in range(1, tpn):
        give(j).start()
    def passed(count):
        arrived(xfar.at[pl.ds(0, chips - 1), pl.ds(0, count)], sent.at[3])
        arrived(xfar.at[pl.ds(0, chips), pl.ds(0, count)], sent.at[4])

    @pl.when(edge)
    def _():
        arrived(xfar.at[0, pl.ds(0, 2 * first)], sent.at[0])
        passed(steps)

    @pl.when(inner)
    def _():
        arrived(xfar.at[0, pl.ds(0, len(raw_to))], sent.at[0])
        arrived(kvs.at[pl.ds(0, len(line_to))], sent.at[6])
        passed(shared)

    arrived(kvs.at[pl.ds(0, half - 1)], sent.at[1])
    arrived(grecv.at[pl.ds(0, n - 1)], sent.at[2])
    arrived(got.at[pl.ds(0, tpn - 1)], sent.at[5])
    arrived(got.at[pl.ds(0, tpn - 1)], recv.at[2])
    total = parts[tp]
    for j in range(1, tpn):
        total = total + got[j]
    read_out[...] = total.astype(BF16)


def publish(count, *refs):
    sources, targets, sems = refs[:count], refs[count : 2 * count], refs[2 * count]
    copies = [
        pltpu.make_async_copy(a, b, sems.at[i]) for i, (a, b) in enumerate(zip(sources, targets))
    ]
    for copy in copies:
        copy.start()
    for copy in copies:
        copy.wait()


def solution(mesh):
    n, tpn = mesh.shape["sp"], mesh.shape["tp"]

    def body(prompt, w_key, w_value, w_in_gate, w_forget_gate, in_bias, forget_bias, query, w_out):
        depth, heads, width = w_key.shape
        seqs = prompt.shape[0] // n
        block = prompt.shape[1]
        rows = seqs * block
        half = n // 2
        chips = tpn // 2
        steps = len(EDGE_TURNS) + len(RAW_TO_END)
        wo = w_out.reshape(heads * width, -1)
        columns = wo.shape[1]
        any_ = pl.BlockSpec(memory_space=pl.ANY)
        vmem = pl.BlockSpec(memory_space=pltpu.VMEM)
        dma = pltpu.SemaphoreType.DMA
        shapes = (
            ((2, seqs, heads, width, width), BF16),
            ((2, seqs, heads, width), F32),
            ((2, heads, seqs), F32),
            ((seqs, columns // tpn), BF16),
        )
        held = pl.pallas_call(
            functools.partial(kernel, n, tpn),
            out_shape=tuple(pltpu.VMEM(*shape) for shape in shapes),
            in_specs=[any_] * 9,
            out_specs=(vmem,) * 4,
            scratch_shapes=[
                pltpu.VMEM((n * seqs, block, depth), BF16),
                pltpu.VMEM((depth, 2 * width), BF16),
                pltpu.VMEM((width, columns), BF16),
                pltpu.VMEM((2, 2, depth), BF16),
                pltpu.VMEM((2, 1, 2), F32),
                pltpu.VMEM((seqs, width), BF16),
                pltpu.VMEM((16, depth), BF16),
                pltpu.VMEM((half + len(LINE_TO_END + LINE_TO_MIDDLE), rows, 2 * width), BF16),
                pltpu.VMEM((half, rows, 2 * width), BF16),
                pltpu.VMEM((half, rows, 2 * width), BF16),
                pltpu.VMEM((n, 4, rows), F32),
                pltpu.VMEM((n, 4, rows), F32),
                pltpu.VMEM((seqs, half, block, depth), BF16),
                pltpu.VMEM((rows, 4 * half), F32),
                pltpu.VMEM((4, seqs, half, block, width), F32),
                pltpu.VMEM((seqs, width, width), F32),
                pltpu.VMEM((seqs, width, 2 * width), F32),
                pltpu.VMEM((2, seqs, width), F32),
                pltpu.VMEM((2, seqs, width), F32),
                pltpu.VMEM((tpn, seqs, columns // tpn), F32),
                pltpu.VMEM((tpn, seqs, columns // tpn), F32),
                dma((9,)),
                dma((steps,)),
                dma((steps,)),
                dma((len(GROUPS),)),
                dma((4,)),
                dma((7,)),
            ],
            compiler_params=pltpu.CompilerParams(collective_id=0, has_side_effects=True),
            name="memories",
        )(
            prompt, w_key.reshape(depth, width), w_value.reshape(depth, width), wo,
            w_in_gate.reshape(2, depth), w_forget_gate.reshape(2, depth),
            in_bias.reshape(1, 2), forget_bias.reshape(1, 2), query.reshape(seqs, width),
        )
        memory, normal, stable, read = pl.pallas_call(
            functools.partial(publish, len(shapes)),
            out_shape=tuple(jax.ShapeDtypeStruct(*shape) for shape in shapes),
            in_specs=[vmem] * len(shapes),
            out_specs=(any_,) * len(shapes),
            scratch_shapes=[dma((len(shapes),))],
            name="outputs",
        )(*[pltpu.with_memory_space_constraint(a, pltpu.VMEM) for a in held])
        return memory, normal, stable.transpose(0, 2, 1), read

    return jax.shard_map(
        body,
        mesh=mesh,
        in_specs=(
            P("gr", "sp", None),
            P(None, "tp", None),
            P(None, "tp", None),
            P(None, None, "tp"),
            P(None, None, "tp"),
            P(None, "tp"),
            P(None, "tp"),
            P(("gr", "sp"), "tp", None),
            P("tp", None, None),
        ),
        out_specs=(
            P(None, ("gr", "sp"), "tp", None, None),
            P(None, ("gr", "sp"), "tp", None),
            P(None, ("gr", "sp"), "tp"),
            P(("gr", "sp"), "tp"),
        ),
        check_vma=False,
    )
```

```python
import functools

import jax
import jax.numpy as jnp
from jax import lax
from jax.experimental import pallas as pl
from jax.experimental.pallas import tpu as pltpu
from jax.sharding import PartitionSpec as P

MESH = pl.DeviceIdType.MESH
F32 = jnp.float32
BF16 = jnp.bfloat16
HIGHEST = lax.Precision.HIGHEST


def nt(a, b):
    return lax.dot_general(a, b, (((1,), (1,)), ((), ())), preferred_element_type=F32)


def tn(a, b):
    return lax.dot_general(a, b, (((0,), (0,)), ((), ())), preferred_element_type=F32)


def iota(shape, axis):
    return lax.broadcasted_iota(jnp.int32, shape, axis)


EDGE_TURNS = (0, 2, 1, 3)
RAW_TO_END, RAW_TO_MIDDLE = (2, 3), (2,)
LINE_TO_END, LINE_TO_MIDDLE = (0, 1), (0, 1, 3)
GROUPS = ((0, 1), (2, 3), (4,), (5,))
FIRST = (
    ("gates", 0),
    ("gates", 1),
    ("barrier", 0),
    ("loaded", 0),
    ("edge", 0),
    ("edge", 1),
    ("inner", 0),
    ("gates", 2),
    ("gates", 3),
    ("send", 0),
    ("weights", 0),
    ("line", 0),
    ("same", 0),
    ("other", 0),
    ("own", 0),
)
ORDER = (
    ("own", 0),
    ("own", 1),
    ("queries", 0),
    ("own", 2),
    ("own", 3),
    ("pass", 0),
    ("own", 4),
    ("pass", 1),
    ("own", 5),
    ("pass", 2),
    ("gates", 0),
    ("pass", 3),
    ("widen", 0),
    ("widen", 1),
    ("widen", 2),
    ("pass", 4),
    ("widen", 3),
    ("collect", 0),
    ("pass", 5),
    ("collect", 1),
    ("collect", 2),
    ("collect", 3),
    ("near", 0),
)


def kernel(
    n, tpn,
    prompt, wk_hbm, wv_hbm, wo_hbm, ig_hbm, fg_hbm, ib_hbm, fb_hbm, q_hbm,
    membuf, norm_out, stab_out, read_out,
    xall, wkv, wo, gate_w, biases, query,
    wg, kvs, kvn, kvf, gsend, grecv, xfar, cols, wb, qb, acc, num, nrm, parts, got,
    lsem, frecv, xrecv, drecv, recv, sent,
):
    sp = lax.axis_index("sp")
    tp = lax.axis_index("tp")
    half = n // 2
    cores = 2
    chips = tpn // cores
    seqs, _, block, depth = xfar.shape
    rows = seqs * block
    width = wo.shape[0]
    line = half // 2
    side = sp // half
    local = sp - side * half
    deck, y = local // line, lax.rem(local, line)
    edge = deck == side
    near_base = side * half
    far_base = half - near_base
    x, c = tp // cores, lax.rem(tp, cores)
    partner = x * cores + 1 - c

    barrier = pltpu.get_barrier_semaphore()
    for i in range(half):
        pl.semaphore_signal(
            barrier,
            inc=1,
            device_id={"sp": far_base + lax.rem(local + half // 2 + i, half)},
            device_id_type=MESH,
        )
    for k in range(1, half):
        pl.semaphore_signal(
            barrier,
            inc=1,
            device_id={"sp": near_base + lax.rem(local + k, half)},
            device_id_type=MESH,
        )
    for j in range(1, tpn):
        pl.semaphore_signal(
            barrier, inc=1, device_id={"tp": lax.rem(tp + j, tpn)}, device_id_type=MESH
        )

    first = len(EDGE_TURNS)
    steps, shared = first + len(RAW_TO_END), first + len(RAW_TO_MIDDLE)

    def far_from(k):
        deck_of = 1 - side if k < first else side
        turn = (EDGE_TURNS + RAW_TO_END)[k]
        return deck_of * line + lax.rem(y + line - turn, line)

    def far_to(near_middle, turn):
        deck_of = side if near_middle else 1 - side
        return far_base + deck_of * line + lax.rem(y + turn, line)

    raw_to = [(False, turn) for turn in RAW_TO_END] + [(True, turn) for turn in RAW_TO_MIDDLE]
    line_to = [(False, turn) for turn in LINE_TO_END] + [(True, turn) for turn in LINE_TO_MIDDLE]

    def near_to(deck_of, turn):
        return deck_of * line + lax.rem(y + turn, line)

    pieces = 4

    def load(i):
        base = (near_base if i < pieces // 2 else far_base) + i % (pieces // 2) * (2 * half // pieces)
        part = pl.ds(base * seqs, 2 * half // pieces * seqs)
        return pltpu.make_async_copy(prompt.at[part], xall.at[part], lsem.at[i])

    gate_loads = [
        pltpu.make_async_copy(ig_hbm, gate_w.at[0], lsem.at[4]),
        pltpu.make_async_copy(fg_hbm, gate_w.at[1], lsem.at[4]),
    ]
    weight_loads = [
        pltpu.make_async_copy(wk_hbm, wkv.at[:, :width], lsem.at[5]),
        pltpu.make_async_copy(wv_hbm, wkv.at[:, width:], lsem.at[5]),
    ]
    late_loads = [
        pltpu.make_async_copy(ib_hbm, biases.at[0], lsem.at[6]),
        pltpu.make_async_copy(fb_hbm, biases.at[1], lsem.at[6]),
        pltpu.make_async_copy(q_hbm, query, lsem.at[7]),
        pltpu.make_async_copy(wo_hbm, wo, lsem.at[8]),
    ]

    def arrived(ref, sem):
        pltpu.make_async_copy(ref, ref, sem).wait()

    def send_far(near_middle, turn, slot):
        dest = far_to(near_middle, turn)
        return pltpu.make_async_remote_copy(
            src_ref=xall.at[dest * seqs + tp],
            dst_ref=xfar.at[tp, local],
            send_sem=sent.at[0],
            recv_sem=frecv.at[slot],
            device_id={"sp": dest},
            device_id_type=MESH,
        )

    def far_from_edge(at):
        for slot, turn in enumerate(EDGE_TURNS):
            send_far(at == 1, turn, slot).start()

    def far_from_inner():
        for i, (near_middle, turn) in enumerate(raw_to):
            send_far(near_middle, turn, first + i % len(RAW_TO_END)).start()

    def send_near(deck_of, turn):
        dest = near_to(deck_of, turn)
        return pltpu.make_async_remote_copy(
            src_ref=kvs.at[dest],
            dst_ref=kvn.at[local],
            send_sem=sent.at[1],
            recv_sem=recv.at[0],
            device_id={"sp": near_base + dest},
            device_id_type=MESH,
        )

    def send_line(i):
        return pltpu.make_async_remote_copy(
            src_ref=kvs.at[half + i],
            dst_ref=kvf.at[local],
            send_sem=sent.at[6],
            recv_sem=recv.at[3],
            device_id={"sp": far_to(*line_to[i])},
            device_id_type=MESH,
        )

    def send_gates(k):
        dest = lax.rem(sp + k, n)
        return pltpu.make_async_remote_copy(
            src_ref=gsend.at[dest],
            dst_ref=grecv.at[sp],
            send_sem=sent.at[2],
            recv_sem=recv.at[1],
            device_id={"sp": dest},
            device_id_type=MESH,
        )

    def spread(j, k):
        piece = xfar.at[tp, far_from(k)]
        return pltpu.make_async_remote_copy(
            src_ref=piece,
            dst_ref=piece,
            send_sem=sent.at[3],
            recv_sem=xrecv.at[k],
            device_id={"tp": lax.rem(x + j, chips) * cores + c},
            device_id_type=MESH,
        )

    def group_of(k):
        return [p for p, group in enumerate(GROUPS) if k in group][0]

    def hand(j, k):
        origin = lax.rem(x + chips - j, chips) * cores + c
        piece = xfar.at[origin, far_from(k)]
        return pltpu.make_async_remote_copy(
            src_ref=piece,
            dst_ref=piece,
            send_sem=sent.at[4],
            recv_sem=drecv.at[group_of(k)],
            device_id={"tp": partner},
            device_id_type=MESH,
        )

    def give(j):
        peer = lax.rem(tp + j, tpn)
        return pltpu.make_async_remote_copy(
            src_ref=parts.at[peer],
            dst_ref=got.at[j],
            send_sem=sent.at[5],
            recv_sem=recv.at[2],
            device_id={"tp": peer},
            device_id_type=MESH,
        )

    for copy in gate_loads:
        copy.start()
    for i in range(pieces):
        load(i).start()
    for copy in weight_loads + late_loads:
        copy.start()

    arrived(gate_w, lsem.at[4])
    wg[...] = jnp.concatenate(
        [gate_w[0].astype(F32), gate_w[1].astype(F32), jnp.zeros((wg.shape[0] - 4, depth), F32)],
        axis=0,
    ).astype(BF16)

    def rows_of(dest):
        return xall[pl.ds(dest * seqs, seqs)].reshape(rows, depth)

    def gates(start, stop):
        for i in range(start, stop):
            if i < half and i % (2 * half // pieces) == 0:
                load(i // (2 * half // pieces)).wait()
            dest = (near_base if i < half else far_base) + i % half
            gsend[pl.ds(dest, 1)] = nt(wg[...], rows_of(dest))[:4][None]

    inner = jnp.logical_not(edge)

    def start_gates():
        grecv[pl.ds(sp, 1)] = gsend[pl.ds(sp, 1)]
        for k in range(1, n):
            send_gates(k).start()

    def keys_values(blocks, base):
        lines = [rows_of(dest) for dest in blocks]
        both = jnp.dot(
            jnp.concatenate(lines, axis=0), wkv[...], preferred_element_type=F32
        ).astype(BF16)
        kvs[pl.ds(base, len(blocks))] = both.reshape(len(blocks), rows, 2 * width)

    def near_other():
        base = (1 - deck) * line
        keys_values([near_base + base + i for i in range(line)], base)
        for turn in (2, 1, 3, 0):
            send_near(1 - deck, turn).start()

    def near_same():
        base = deck * line
        keys_values([near_base + base + i for i in range(line)], base)
        for turn in (2, 1, 3):
            send_near(deck, turn).start()

    def own_near():
        kvn[pl.ds(local, 1)] = kvs[pl.ds(local, 1)]

    def lines():
        count = len(line_to)
        keys_values([far_to(*to) for to in line_to], half)
        for i in range(count):
            send_line(i).start()

    first_jobs = {
        "barrier": lambda _: pl.semaphore_wait(barrier, n - 1 + tpn - 1),
        "loaded": lambda _: [load(i).wait() for i in range(pieces // 2, pieces)],
        "edge": lambda at: pl.when(edge)(functools.partial(far_from_edge, at)),
        "inner": lambda _: pl.when(inner)(far_from_inner),
        "gates": lambda at: gates(at * half // 2, (at + 1) * half // 2),
        "send": lambda _: start_gates(),
        "weights": lambda _: arrived(wkv, lsem.at[5]),
        "other": lambda _: near_other(),
        "same": lambda _: near_same(),
        "own": lambda _: own_near(),
        "line": lambda _: pl.when(inner)(lines),
    }
    for job, at in FIRST:
        first_jobs[job](at)

    def weigh():
        lane = iota((rows, rows), 1)
        down = iota((rows, rows), 0)
        same = (lane // block) == (down // block)
        upto = (same & (down <= lane)).astype(F32)
        whole = same.astype(F32)
        before = (
            (iota((2 * n, 2 * n), 0) // n == iota((2 * n, 2 * n), 1) // n)
            & (iota((2 * n, 2 * n), 1) < iota((2 * n, 2 * n), 0))
        ).astype(F32)
        pre = [
            grecv[:, i, :] + biases[i // 2, 0:1, i % 2 : i % 2 + 1]
            for i in range(4)
        ]
        forget_pre = jnp.concatenate(pre[2:], axis=0)
        forget = jnp.minimum(forget_pre, 0.0) - jnp.log1p(jnp.exp(-jnp.abs(forget_pre)))
        inside = jnp.dot(forget, upto, preferred_element_type=F32, precision=HIGHEST)
        sums = jnp.dot(forget, whole, preferred_element_type=F32, precision=HIGHEST)
        running = jnp.dot(before, sums, preferred_element_type=F32, precision=HIGHEST) + inside
        totals = [jnp.sum(sums[g * n : (g + 1) * n], axis=0, keepdims=True) for g in range(2)]
        logs = [
            pre[0] + totals[0] - running[:n],
            pre[1] + running[n:] - forget[n:],
        ]
        peak = jnp.concatenate(
            [jnp.maximum(totals[g], jnp.max(logs[g], axis=0, keepdims=True)) for g in range(2)]
            + [jnp.zeros((6, rows), F32)],
            axis=0,
        )
        spot = iota(peak.shape, 1)
        step = 1
        while step < block:
            low, high = pltpu.roll(peak, step, 1), pltpu.roll(peak, rows - step, 1)
            peak = jnp.maximum(peak, jnp.where((spot & step) != 0, low, high))
            step *= 2
        weight = [jnp.exp(logs[g] - peak[g : g + 1]) * width ** (-0.5) for g in range(2)]
        first = side == 0
        parted = [jnp.where(first, w[:half], w[half:]) for w in weight]
        parted += [jnp.where(first, w[half:], w[:half]) for w in weight]
        cols[...] = jnp.concatenate(parted, axis=0).T
        own = iota((seqs, rows), 1) // block == iota((seqs, rows), 0)
        return [
            jnp.max(jnp.where(own, peak[g : g + 1], -jnp.inf), axis=1, keepdims=True)
            for g in range(2)
        ]

    def widen(i):
        for q in range(seqs):
            for s in range(half):
                j = i * half + s
                wb[i, q, s] = jnp.broadcast_to(
                    cols[q * block : (q + 1) * block, j : j + 1], (block, width)
                )

    def outer(kv, i, q):
        lines = slice(q * block, (q + 1) * block)
        keys = kv[:, lines, :width].reshape(half * block, width)
        values = kv[:, lines, width:].reshape(half * block, width).astype(F32)
        w0 = wb[2 * i, q].reshape(half * block, width)
        w1 = wb[2 * i + 1, q].reshape(half * block, width)
        weighted = jnp.concatenate([values * w0, values * w1], axis=1).astype(BF16)
        keys_f = keys.astype(F32)
        sums = [jnp.sum(keys_f * w, axis=0, keepdims=True) for w in (w0, w1)]
        return tn(keys, weighted), sums

    def project(p):
        found = [far_from(k) for k in GROUPS[p]]
        lines = [xfar[:, pl.ds(source, 1)].reshape(rows, depth) for source in found]
        both = jnp.dot(
            jnp.concatenate(lines, axis=0), wkv[...], preferred_element_type=F32
        ).astype(BF16)
        for i, source in enumerate(found):
            kvf[pl.ds(source, 1)] = both[i * rows : (i + 1) * rows][None]

    def own(k):
        arrived(xfar.at[0, 0], frecv.at[k])
        for j in (2, 1, 3):
            spread(j, k).start()
        hand(0, k).start()

    def pass_on(k):
        arrived(xfar.at[pl.ds(1, chips - 1), 0], xrecv.at[k])
        for j in (1, 3, 2):
            hand(j, k).start()

    def collect(p):
        arrived(xfar.at[pl.ds(0, chips), pl.ds(0, len(GROUPS[p]))], drecv.at[p])
        project(p)

    def queries():
        arrived(biases, lsem.at[6])
        for copy in late_loads[2:]:
            copy.wait()
        turned = query[...].astype(F32).T
        for q in range(seqs):
            qb[q] = jnp.broadcast_to(turned[:, q : q + 1], (width, width))

    stables = []

    def gates_in():
        arrived(grecv.at[pl.ds(0, n - 1)], recv.at[1])
        stables.extend(weigh())

    def widened(i):
        widen(i)

    def near_part():
        arrived(kvn.at[pl.ds(0, half - 1)], recv.at[0])
        for q in range(seqs):
            acc[q], sums = outer(kvn, 0, q)
            for g in range(2):
                nrm[g, q : q + 1] = sums[g]

    jobs = {
        "own": own, "pass": pass_on, "collect": collect, "widen": widened,
        "queries": lambda _: queries(), "gates": lambda _: gates_in(), "near": lambda _: near_part(),
    }
    for job, at in ORDER:
        slot = GROUPS[at][0] if job == "collect" else at if job in ("own", "pass") else 0
        if slot < shared:
            jobs[job](at)
        else:
            pl.when(edge)(functools.partial(jobs[job], at))
    @pl.when(edge)
    def _():
        arrived(kvf.at[pl.ds(0, len(LINE_TO_END))], recv.at[3])

    @pl.when(inner)
    def _():
        arrived(kvf.at[pl.ds(0, len(LINE_TO_MIDDLE))], recv.at[3])

    for q in range(seqs):
        more, sums = outer(kvf, 1, q)
        memory = (acc[q] + more).astype(BF16)
        back = memory.astype(F32)
        for g in range(2):
            membuf[g, q, 0] = memory[:, g * width : (g + 1) * width]
            num[g, q : q + 1] = jnp.sum(
                qb[q] * back[:, g * width : (g + 1) * width], axis=0, keepdims=True
            )
            total = nrm[g, q : q + 1] + sums[g]
            nrm[g, q : q + 1] = total
            norm_out[g, q] = total

    hidden = jnp.zeros((seqs, width), F32)
    queries = query[...].astype(F32)
    for g in range(2):
        under = jnp.abs(jnp.sum(queries * nrm[g], axis=1, keepdims=True))
        floor = jnp.maximum(jnp.exp(-stables[g]), 1.0)
        hidden = hidden + num[g] / jnp.maximum(under, floor)
        square = iota((seqs, width), 1) == iota((seqs, width), 0)
        row = jnp.sum(jnp.where(square, stables[g], 0.0), axis=0, keepdims=True)
        stab_out[g] = row[:, :seqs]
    terms = jnp.dot(hidden.astype(BF16), wo[...], preferred_element_type=F32)
    share = terms.shape[1] // tpn
    for t in range(tpn):
        parts[t] = terms[:, t * share : (t + 1) * share]
    for j in sorted(range(1, tpn), key=lambda j: abs(j - tpn / 2)):
        give(j).start()
    def passed(count):
        arrived(xfar.at[pl.ds(0, chips - 1), pl.ds(0, count)], sent.at[3])
        arrived(xfar.at[pl.ds(0, chips), pl.ds(0, count)], sent.at[4])

    @pl.when(edge)
    def _():
        arrived(xfar.at[0, pl.ds(0, 2 * first)], sent.at[0])
        passed(steps)

    @pl.when(inner)
    def _():
        arrived(xfar.at[0, pl.ds(0, len(raw_to))], sent.at[0])
        arrived(kvs.at[pl.ds(0, len(line_to))], sent.at[6])
        passed(shared)

    arrived(kvs.at[pl.ds(0, half - 1)], sent.at[1])
    arrived(grecv.at[pl.ds(0, n - 1)], sent.at[2])
    arrived(got.at[pl.ds(0, tpn - 1)], sent.at[5])
    arrived(got.at[pl.ds(0, tpn - 1)], recv.at[2])
    total = parts[tp]
    for j in range(1, tpn):
        total = total + got[j]
    read_out[...] = total.astype(BF16)


def publish(count, *refs):
    sources, targets, sems = refs[:count], refs[count : 2 * count], refs[2 * count]
    copies = [
        pltpu.make_async_copy(a, b, sems.at[i]) for i, (a, b) in enumerate(zip(sources, targets))
    ]
    for copy in copies:
        copy.start()
    for copy in copies:
        copy.wait()


def solution(mesh):
    n, tpn = mesh.shape["sp"], mesh.shape["tp"]

    def body(prompt, w_key, w_value, w_in_gate, w_forget_gate, in_bias, forget_bias, query, w_out):
        depth, heads, width = w_key.shape
        seqs = prompt.shape[0] // n
        block = prompt.shape[1]
        rows = seqs * block
        half = n // 2
        chips = tpn // 2
        steps = len(EDGE_TURNS) + len(RAW_TO_END)
        wo = w_out.reshape(heads * width, -1)
        columns = wo.shape[1]
        any_ = pl.BlockSpec(memory_space=pl.ANY)
        vmem = pl.BlockSpec(memory_space=pltpu.VMEM)
        dma = pltpu.SemaphoreType.DMA
        shapes = (
            ((2, seqs, heads, width, width), BF16),
            ((2, seqs, heads, width), F32),
            ((2, heads, seqs), F32),
            ((seqs, columns // tpn), BF16),
        )
        held = pl.pallas_call(
            functools.partial(kernel, n, tpn),
            out_shape=tuple(pltpu.VMEM(*shape) for shape in shapes),
            in_specs=[any_] * 9,
            out_specs=(vmem,) * 4,
            scratch_shapes=[
                pltpu.VMEM((n * seqs, block, depth), BF16),
                pltpu.VMEM((depth, 2 * width), BF16),
                pltpu.VMEM((width, columns), BF16),
                pltpu.VMEM((2, 2, depth), BF16),
                pltpu.VMEM((2, 1, 2), F32),
                pltpu.VMEM((seqs, width), BF16),
                pltpu.VMEM((16, depth), BF16),
                pltpu.VMEM((half + len(LINE_TO_END + LINE_TO_MIDDLE), rows, 2 * width), BF16),
                pltpu.VMEM((half, rows, 2 * width), BF16),
                pltpu.VMEM((half, rows, 2 * width), BF16),
                pltpu.VMEM((n, 4, rows), F32),
                pltpu.VMEM((n, 4, rows), F32),
                pltpu.VMEM((seqs, half, block, depth), BF16),
                pltpu.VMEM((rows, 4 * half), F32),
                pltpu.VMEM((4, seqs, half, block, width), F32),
                pltpu.VMEM((seqs, width, width), F32),
                pltpu.VMEM((seqs, width, 2 * width), F32),
                pltpu.VMEM((2, seqs, width), F32),
                pltpu.VMEM((2, seqs, width), F32),
                pltpu.VMEM((tpn, seqs, columns // tpn), F32),
                pltpu.VMEM((tpn, seqs, columns // tpn), F32),
                dma((9,)),
                dma((steps,)),
                dma((steps,)),
                dma((len(GROUPS),)),
                dma((4,)),
                dma((7,)),
            ],
            compiler_params=pltpu.CompilerParams(collective_id=0, has_side_effects=True),
            name="memories",
        )(
            prompt, w_key.reshape(depth, width), w_value.reshape(depth, width), wo,
            w_in_gate.reshape(2, depth), w_forget_gate.reshape(2, depth),
            in_bias.reshape(1, 2), forget_bias.reshape(1, 2), query.reshape(seqs, width),
        )
        memory, normal, stable, read = pl.pallas_call(
            functools.partial(publish, len(shapes)),
            out_shape=tuple(jax.ShapeDtypeStruct(*shape) for shape in shapes),
            in_specs=[vmem] * len(shapes),
            out_specs=(any_,) * len(shapes),
            scratch_shapes=[dma((len(shapes),))],
            name="outputs",
        )(*[pltpu.with_memory_space_constraint(a, pltpu.VMEM) for a in held])
        return memory, normal, stable.transpose(0, 2, 1), read

    return jax.shard_map(
        body,
        mesh=mesh,
        in_specs=(
            P("gr", "sp", None),
            P(None, "tp", None),
            P(None, "tp", None),
            P(None, None, "tp"),
            P(None, None, "tp"),
            P(None, "tp"),
            P(None, "tp"),
            P(("gr", "sp"), "tp", None),
            P("tp", None, None),
        ),
        out_specs=(
            P(None, ("gr", "sp"), "tp", None, None),
            P(None, ("gr", "sp"), "tp", None),
            P(None, ("gr", "sp"), "tp"),
            P(("gr", "sp"), "tp"),
        ),
        check_vma=False,
    )
```

```python
import functools

import jax
import jax.numpy as jnp
from jax import lax
from jax.experimental import pallas as pl
from jax.experimental.pallas import tpu as pltpu
from jax.sharding import PartitionSpec as P

MESH = pl.DeviceIdType.MESH
F32 = jnp.float32
BF16 = jnp.bfloat16
HIGHEST = lax.Precision.HIGHEST


def nt(a, b):
    return lax.dot_general(a, b, (((1,), (1,)), ((), ())), preferred_element_type=F32)


def tn(a, b):
    return lax.dot_general(a, b, (((0,), (0,)), ((), ())), preferred_element_type=F32)


def iota(shape, axis):
    return lax.broadcasted_iota(jnp.int32, shape, axis)


EDGE_TURNS = (0, 2, 1, 3)
RAW_TO_END, RAW_TO_MIDDLE = (2, 3), (2,)
LINE_TO_END, LINE_TO_MIDDLE = (0, 1), (0, 1, 3)
GROUPS = ((0, 1), (2, 3), (4,), (5,))
FIRST = (
    ("gates", 0),
    ("gates", 1),
    ("barrier", 0),
    ("loaded", 0),
    ("edge", 0),
    ("edge", 1),
    ("inner", 0),
    ("gates", 2),
    ("gates", 3),
    ("send", 0),
    ("weights", 0),
    ("line", 0),
    ("same", 0),
    ("other", 0),
    ("own", 0),
)
ORDER = (
    ("own", 0),
    ("own", 1),
    ("queries", 0),
    ("own", 2),
    ("own", 3),
    ("pass", 0),
    ("own", 4),
    ("pass", 1),
    ("own", 5),
    ("pass", 2),
    ("gates", 0),
    ("pass", 3),
    ("widen", 0),
    ("widen", 1),
    ("widen", 2),
    ("pass", 4),
    ("widen", 3),
    ("collect", 0),
    ("pass", 5),
    ("collect", 1),
    ("collect", 2),
    ("collect", 3),
    ("near", 0),
)


def kernel(
    n, tpn,
    prompt, wk_hbm, wv_hbm, wo_hbm, ig_hbm, fg_hbm, ib_hbm, fb_hbm, q_hbm,
    membuf, norm_out, stab_out, read_out,
    xall, wkv, wo, gate_w, biases, query,
    wg, kvs, kvn, kvf, gsend, grecv, xfar, cols, wb, qb, acc, num, nrm, parts, got,
    lsem, frecv, xrecv, drecv, recv, sent,
):
    sp = lax.axis_index("sp")
    tp = lax.axis_index("tp")
    half = n // 2
    cores = 2
    chips = tpn // cores
    seqs, _, block, depth = xfar.shape
    rows = seqs * block
    width = wo.shape[0]
    line = half // 2
    side = sp // half
    local = sp - side * half
    deck, y = local // line, lax.rem(local, line)
    edge = deck == side
    near_base = side * half
    far_base = half - near_base
    x, c = tp // cores, lax.rem(tp, cores)
    partner = x * cores + 1 - c

    barrier = pltpu.get_barrier_semaphore()
    for i in range(half):
        pl.semaphore_signal(
            barrier,
            inc=1,
            device_id={"sp": far_base + lax.rem(local + half // 2 + i, half)},
            device_id_type=MESH,
        )
    for k in range(1, half):
        pl.semaphore_signal(
            barrier,
            inc=1,
            device_id={"sp": near_base + lax.rem(local + k, half)},
            device_id_type=MESH,
        )
    for j in range(1, tpn):
        pl.semaphore_signal(
            barrier, inc=1, device_id={"tp": lax.rem(tp + j, tpn)}, device_id_type=MESH
        )

    first = len(EDGE_TURNS)
    steps, shared = first + len(RAW_TO_END), first + len(RAW_TO_MIDDLE)

    def far_from(k):
        deck_of = 1 - side if k < first else side
        turn = (EDGE_TURNS + RAW_TO_END)[k]
        return deck_of * line + lax.rem(y + line - turn, line)

    def far_to(near_middle, turn):
        deck_of = side if near_middle else 1 - side
        return far_base + deck_of * line + lax.rem(y + turn, line)

    raw_to = [(False, turn) for turn in RAW_TO_END] + [(True, turn) for turn in RAW_TO_MIDDLE]
    line_to = [(False, turn) for turn in LINE_TO_END] + [(True, turn) for turn in LINE_TO_MIDDLE]

    def near_to(deck_of, turn):
        return deck_of * line + lax.rem(y + turn, line)

    pieces = 4

    def load(i):
        base = (near_base if i < pieces // 2 else far_base) + i % (pieces // 2) * (2 * half // pieces)
        part = pl.ds(base * seqs, 2 * half // pieces * seqs)
        return pltpu.make_async_copy(prompt.at[part], xall.at[part], lsem.at[i])

    gate_loads = [
        pltpu.make_async_copy(ig_hbm, gate_w.at[0], lsem.at[4]),
        pltpu.make_async_copy(fg_hbm, gate_w.at[1], lsem.at[4]),
    ]
    weight_loads = [
        pltpu.make_async_copy(wk_hbm, wkv.at[:, :width], lsem.at[5]),
        pltpu.make_async_copy(wv_hbm, wkv.at[:, width:], lsem.at[5]),
    ]
    late_loads = [
        pltpu.make_async_copy(ib_hbm, biases.at[0], lsem.at[6]),
        pltpu.make_async_copy(fb_hbm, biases.at[1], lsem.at[6]),
        pltpu.make_async_copy(q_hbm, query, lsem.at[7]),
        pltpu.make_async_copy(wo_hbm, wo, lsem.at[8]),
    ]

    def arrived(ref, sem):
        pltpu.make_async_copy(ref, ref, sem).wait()

    def send_far(near_middle, turn, slot):
        dest = far_to(near_middle, turn)
        return pltpu.make_async_remote_copy(
            src_ref=xall.at[dest * seqs + tp],
            dst_ref=xfar.at[tp, local],
            send_sem=sent.at[0],
            recv_sem=frecv.at[slot],
            device_id={"sp": dest},
            device_id_type=MESH,
        )

    def far_from_edge(at):
        for slot, turn in enumerate(EDGE_TURNS):
            send_far(at == 1, turn, slot).start()

    def far_from_inner():
        for i, (near_middle, turn) in enumerate(raw_to):
            send_far(near_middle, turn, first + i % len(RAW_TO_END)).start()

    def send_near(deck_of, turn):
        dest = near_to(deck_of, turn)
        return pltpu.make_async_remote_copy(
            src_ref=kvs.at[dest],
            dst_ref=kvn.at[local],
            send_sem=sent.at[1],
            recv_sem=recv.at[0],
            device_id={"sp": near_base + dest},
            device_id_type=MESH,
        )

    def send_line(i):
        return pltpu.make_async_remote_copy(
            src_ref=kvs.at[half + i],
            dst_ref=kvf.at[local],
            send_sem=sent.at[6],
            recv_sem=recv.at[3],
            device_id={"sp": far_to(*line_to[i])},
            device_id_type=MESH,
        )

    def send_gates(k):
        dest = lax.rem(sp + k, n)
        return pltpu.make_async_remote_copy(
            src_ref=gsend.at[dest],
            dst_ref=grecv.at[sp],
            send_sem=sent.at[2],
            recv_sem=recv.at[1],
            device_id={"sp": dest},
            device_id_type=MESH,
        )

    def spread(j, k):
        piece = xfar.at[tp, far_from(k)]
        return pltpu.make_async_remote_copy(
            src_ref=piece,
            dst_ref=piece,
            send_sem=sent.at[3],
            recv_sem=xrecv.at[k],
            device_id={"tp": lax.rem(x + j, chips) * cores + c},
            device_id_type=MESH,
        )

    def group_of(k):
        return [p for p, group in enumerate(GROUPS) if k in group][0]

    def hand(j, k):
        origin = lax.rem(x + chips - j, chips) * cores + c
        piece = xfar.at[origin, far_from(k)]
        return pltpu.make_async_remote_copy(
            src_ref=piece,
            dst_ref=piece,
            send_sem=sent.at[4],
            recv_sem=drecv.at[group_of(k)],
            device_id={"tp": partner},
            device_id_type=MESH,
        )

    def give(j):
        peer = lax.rem(tp + j, tpn)
        return pltpu.make_async_remote_copy(
            src_ref=parts.at[peer],
            dst_ref=got.at[j],
            send_sem=sent.at[5],
            recv_sem=recv.at[2],
            device_id={"tp": peer},
            device_id_type=MESH,
        )

    for copy in gate_loads:
        copy.start()
    for i in range(pieces):
        load(i).start()
    for copy in weight_loads + late_loads:
        copy.start()

    arrived(gate_w, lsem.at[4])
    wg[...] = jnp.concatenate(
        [gate_w[0].astype(F32), gate_w[1].astype(F32), jnp.zeros((wg.shape[0] - 4, depth), F32)],
        axis=0,
    ).astype(BF16)

    def rows_of(dest):
        return xall[pl.ds(dest * seqs, seqs)].reshape(rows, depth)

    def gates(start, stop):
        for i in range(start, stop):
            if i < half and i % (2 * half // pieces) == 0:
                load(i // (2 * half // pieces)).wait()
            dest = (near_base if i < half else far_base) + i % half
            gsend[pl.ds(dest, 1)] = nt(wg[...], rows_of(dest))[:4][None]

    inner = jnp.logical_not(edge)

    def start_gates():
        grecv[pl.ds(sp, 1)] = gsend[pl.ds(sp, 1)]
        for k in range(1, n):
            send_gates(k).start()

    def keys_values(blocks, base):
        lines = [rows_of(dest) for dest in blocks]
        both = jnp.dot(
            jnp.concatenate(lines, axis=0), wkv[...], preferred_element_type=F32
        ).astype(BF16)
        kvs[pl.ds(base, len(blocks))] = both.reshape(len(blocks), rows, 2 * width)

    def near_other():
        base = (1 - deck) * line
        keys_values([near_base + base + i for i in range(line)], base)
        for turn in (2, 1, 3, 0):
            send_near(1 - deck, turn).start()

    def near_same():
        base = deck * line
        keys_values([near_base + base + i for i in range(line)], base)
        for turn in (2, 1, 3):
            send_near(deck, turn).start()

    def own_near():
        kvn[pl.ds(local, 1)] = kvs[pl.ds(local, 1)]

    def lines():
        count = len(line_to)
        keys_values([far_to(*to) for to in line_to], half)
        for i in range(count):
            send_line(i).start()

    first_jobs = {
        "barrier": lambda _: pl.semaphore_wait(barrier, n - 1 + tpn - 1),
        "loaded": lambda _: [load(i).wait() for i in range(pieces // 2, pieces)],
        "edge": lambda at: pl.when(edge)(functools.partial(far_from_edge, at)),
        "inner": lambda _: pl.when(inner)(far_from_inner),
        "gates": lambda at: gates(at * half // 2, (at + 1) * half // 2),
        "send": lambda _: start_gates(),
        "weights": lambda _: arrived(wkv, lsem.at[5]),
        "other": lambda _: near_other(),
        "same": lambda _: near_same(),
        "own": lambda _: own_near(),
        "line": lambda _: pl.when(inner)(lines),
    }
    for job, at in FIRST:
        first_jobs[job](at)

    def weigh():
        lane = iota((rows, rows), 1)
        down = iota((rows, rows), 0)
        same = (lane // block) == (down // block)
        upto = (same & (down <= lane)).astype(F32)
        whole = same.astype(F32)
        before = (
            (iota((2 * n, 2 * n), 0) // n == iota((2 * n, 2 * n), 1) // n)
            & (iota((2 * n, 2 * n), 1) < iota((2 * n, 2 * n), 0))
        ).astype(F32)
        pre = [
            grecv[:, i, :] + biases[i // 2, 0:1, i % 2 : i % 2 + 1]
            for i in range(4)
        ]
        forget_pre = jnp.concatenate(pre[2:], axis=0)
        forget = jnp.minimum(forget_pre, 0.0) - jnp.log1p(jnp.exp(-jnp.abs(forget_pre)))
        inside = jnp.dot(forget, upto, preferred_element_type=F32, precision=HIGHEST)
        sums = jnp.dot(forget, whole, preferred_element_type=F32, precision=HIGHEST)
        running = jnp.dot(before, sums, preferred_element_type=F32, precision=HIGHEST) + inside
        totals = [jnp.sum(sums[g * n : (g + 1) * n], axis=0, keepdims=True) for g in range(2)]
        logs = [
            pre[0] + totals[0] - running[:n],
            pre[1] + running[n:] - forget[n:],
        ]
        peak = jnp.concatenate(
            [jnp.maximum(totals[g], jnp.max(logs[g], axis=0, keepdims=True)) for g in range(2)]
            + [jnp.zeros((6, rows), F32)],
            axis=0,
        )
        spot = iota(peak.shape, 1)
        step = 1
        while step < block:
            low, high = pltpu.roll(peak, step, 1), pltpu.roll(peak, rows - step, 1)
            peak = jnp.maximum(peak, jnp.where((spot & step) != 0, low, high))
            step *= 2
        weight = [jnp.exp(logs[g] - peak[g : g + 1]) * width ** (-0.5) for g in range(2)]
        first = side == 0
        parted = [jnp.where(first, w[:half], w[half:]) for w in weight]
        parted += [jnp.where(first, w[half:], w[:half]) for w in weight]
        cols[...] = jnp.concatenate(parted, axis=0).T
        own = iota((seqs, rows), 1) // block == iota((seqs, rows), 0)
        return [
            jnp.max(jnp.where(own, peak[g : g + 1], -jnp.inf), axis=1, keepdims=True)
            for g in range(2)
        ]

    def widen(i):
        for q in range(seqs):
            for s in range(half):
                j = i * half + s
                wb[i, q, s] = jnp.broadcast_to(
                    cols[q * block : (q + 1) * block, j : j + 1], (block, width)
                )

    def outer(kv, i, q):
        lines = slice(q * block, (q + 1) * block)
        keys = kv[:, lines, :width].reshape(half * block, width)
        values = kv[:, lines, width:].reshape(half * block, width).astype(F32)
        w0 = wb[2 * i, q].reshape(half * block, width)
        w1 = wb[2 * i + 1, q].reshape(half * block, width)
        weighted = jnp.concatenate([values * w0, values * w1], axis=1).astype(BF16)
        keys_f = keys.astype(F32)
        sums = [jnp.sum(keys_f * w, axis=0, keepdims=True) for w in (w0, w1)]
        return tn(keys, weighted), sums

    def project(p):
        found = [far_from(k) for k in GROUPS[p]]
        lines = [xfar[:, pl.ds(source, 1)].reshape(rows, depth) for source in found]
        both = jnp.dot(
            jnp.concatenate(lines, axis=0), wkv[...], preferred_element_type=F32
        ).astype(BF16)
        for i, source in enumerate(found):
            kvf[pl.ds(source, 1)] = both[i * rows : (i + 1) * rows][None]

    def own(k):
        arrived(xfar.at[0, 0], frecv.at[k])
        for j in (2, 1, 3):
            spread(j, k).start()
        hand(0, k).start()

    def pass_on(k):
        arrived(xfar.at[pl.ds(1, chips - 1), 0], xrecv.at[k])
        for j in (1, 3, 2):
            hand(j, k).start()

    def collect(p):
        arrived(xfar.at[pl.ds(0, chips), pl.ds(0, len(GROUPS[p]))], drecv.at[p])
        project(p)

    def queries():
        arrived(biases, lsem.at[6])
        for copy in late_loads[2:]:
            copy.wait()
        turned = query[...].astype(F32).T
        for q in range(seqs):
            qb[q] = jnp.broadcast_to(turned[:, q : q + 1], (width, width))

    stables = []

    def gates_in():
        arrived(grecv.at[pl.ds(0, n - 1)], recv.at[1])
        stables.extend(weigh())

    def widened(i):
        widen(i)

    def near_part():
        arrived(kvn.at[pl.ds(0, half - 1)], recv.at[0])
        for q in range(seqs):
            acc[q], sums = outer(kvn, 0, q)
            for g in range(2):
                nrm[g, q : q + 1] = sums[g]

    jobs = {
        "own": own, "pass": pass_on, "collect": collect, "widen": widened,
        "queries": lambda _: queries(), "gates": lambda _: gates_in(), "near": lambda _: near_part(),
    }
    for job, at in ORDER:
        slot = GROUPS[at][0] if job == "collect" else at if job in ("own", "pass") else 0
        if slot < shared:
            jobs[job](at)
        else:
            pl.when(edge)(functools.partial(jobs[job], at))
    @pl.when(edge)
    def _():
        arrived(kvf.at[pl.ds(0, len(LINE_TO_END))], recv.at[3])

    @pl.when(inner)
    def _():
        arrived(kvf.at[pl.ds(0, len(LINE_TO_MIDDLE))], recv.at[3])

    for q in range(seqs):
        more, sums = outer(kvf, 1, q)
        memory = (acc[q] + more).astype(BF16)
        back = memory.astype(F32)
        for g in range(2):
            membuf[g, q, 0] = memory[:, g * width : (g + 1) * width]
            num[g, q : q + 1] = jnp.sum(
                qb[q] * back[:, g * width : (g + 1) * width], axis=0, keepdims=True
            )
            total = nrm[g, q : q + 1] + sums[g]
            nrm[g, q : q + 1] = total
            norm_out[g, q] = total

    hidden = jnp.zeros((seqs, width), F32)
    queries = query[...].astype(F32)
    for g in range(2):
        under = jnp.abs(jnp.sum(queries * nrm[g], axis=1, keepdims=True))
        floor = jnp.maximum(jnp.exp(-stables[g]), 1.0)
        hidden = hidden + num[g] / jnp.maximum(under, floor)
    terms = jnp.dot(hidden.astype(BF16), wo[...], preferred_element_type=F32)
    share = terms.shape[1] // tpn
    for t in range(tpn):
        parts[t] = terms[:, t * share : (t + 1) * share]
    for j in sorted(range(1, tpn), key=lambda j: abs(j - tpn / 2)):
        give(j).start()
    for g in range(2):
        square = iota((seqs, width), 1) == iota((seqs, width), 0)
        row = jnp.sum(jnp.where(square, stables[g], 0.0), axis=0, keepdims=True)
        stab_out[g] = row[:, :seqs]
    def passed(count):
        arrived(xfar.at[pl.ds(0, chips - 1), pl.ds(0, count)], sent.at[3])
        arrived(xfar.at[pl.ds(0, chips), pl.ds(0, count)], sent.at[4])

    @pl.when(edge)
    def _():
        arrived(xfar.at[0, pl.ds(0, 2 * first)], sent.at[0])
        passed(steps)

    @pl.when(inner)
    def _():
        arrived(xfar.at[0, pl.ds(0, len(raw_to))], sent.at[0])
        arrived(kvs.at[pl.ds(0, len(line_to))], sent.at[6])
        passed(shared)

    arrived(kvs.at[pl.ds(0, half - 1)], sent.at[1])
    arrived(grecv.at[pl.ds(0, n - 1)], sent.at[2])
    arrived(got.at[pl.ds(0, tpn - 1)], sent.at[5])
    arrived(got.at[pl.ds(0, tpn - 1)], recv.at[2])
    total = parts[tp]
    for j in range(1, tpn):
        total = total + got[j]
    read_out[...] = total.astype(BF16)


def publish(count, *refs):
    sources, targets, sems = refs[:count], refs[count : 2 * count], refs[2 * count]
    copies = [
        pltpu.make_async_copy(a, b, sems.at[i]) for i, (a, b) in enumerate(zip(sources, targets))
    ]
    for copy in copies:
        copy.start()
    for copy in copies:
        copy.wait()


def solution(mesh):
    n, tpn = mesh.shape["sp"], mesh.shape["tp"]

    def body(prompt, w_key, w_value, w_in_gate, w_forget_gate, in_bias, forget_bias, query, w_out):
        depth, heads, width = w_key.shape
        seqs = prompt.shape[0] // n
        block = prompt.shape[1]
        rows = seqs * block
        half = n // 2
        chips = tpn // 2
        steps = len(EDGE_TURNS) + len(RAW_TO_END)
        wo = w_out.reshape(heads * width, -1)
        columns = wo.shape[1]
        any_ = pl.BlockSpec(memory_space=pl.ANY)
        vmem = pl.BlockSpec(memory_space=pltpu.VMEM)
        dma = pltpu.SemaphoreType.DMA
        shapes = (
            ((2, seqs, heads, width, width), BF16),
            ((2, seqs, heads, width), F32),
            ((2, heads, seqs), F32),
            ((seqs, columns // tpn), BF16),
        )
        held = pl.pallas_call(
            functools.partial(kernel, n, tpn),
            out_shape=tuple(pltpu.VMEM(*shape) for shape in shapes),
            in_specs=[any_] * 9,
            out_specs=(vmem,) * 4,
            scratch_shapes=[
                pltpu.VMEM((n * seqs, block, depth), BF16),
                pltpu.VMEM((depth, 2 * width), BF16),
                pltpu.VMEM((width, columns), BF16),
                pltpu.VMEM((2, 2, depth), BF16),
                pltpu.VMEM((2, 1, 2), F32),
                pltpu.VMEM((seqs, width), BF16),
                pltpu.VMEM((16, depth), BF16),
                pltpu.VMEM((half + len(LINE_TO_END + LINE_TO_MIDDLE), rows, 2 * width), BF16),
                pltpu.VMEM((half, rows, 2 * width), BF16),
                pltpu.VMEM((half, rows, 2 * width), BF16),
                pltpu.VMEM((n, 4, rows), F32),
                pltpu.VMEM((n, 4, rows), F32),
                pltpu.VMEM((seqs, half, block, depth), BF16),
                pltpu.VMEM((rows, 4 * half), F32),
                pltpu.VMEM((4, seqs, half, block, width), F32),
                pltpu.VMEM((seqs, width, width), F32),
                pltpu.VMEM((seqs, width, 2 * width), F32),
                pltpu.VMEM((2, seqs, width), F32),
                pltpu.VMEM((2, seqs, width), F32),
                pltpu.VMEM((tpn, seqs, columns // tpn), F32),
                pltpu.VMEM((tpn, seqs, columns // tpn), F32),
                dma((9,)),
                dma((steps,)),
                dma((steps,)),
                dma((len(GROUPS),)),
                dma((4,)),
                dma((7,)),
            ],
            compiler_params=pltpu.CompilerParams(collective_id=0, has_side_effects=True),
            name="memories",
        )(
            prompt, w_key.reshape(depth, width), w_value.reshape(depth, width), wo,
            w_in_gate.reshape(2, depth), w_forget_gate.reshape(2, depth),
            in_bias.reshape(1, 2), forget_bias.reshape(1, 2), query.reshape(seqs, width),
        )
        memory, normal, stable, read = pl.pallas_call(
            functools.partial(publish, len(shapes)),
            out_shape=tuple(jax.ShapeDtypeStruct(*shape) for shape in shapes),
            in_specs=[vmem] * len(shapes),
            out_specs=(any_,) * len(shapes),
            scratch_shapes=[dma((len(shapes),))],
            name="outputs",
        )(*[pltpu.with_memory_space_constraint(a, pltpu.VMEM) for a in held])
        return memory, normal, stable.transpose(0, 2, 1), read

    return jax.shard_map(
        body,
        mesh=mesh,
        in_specs=(
            P("gr", "sp", None),
            P(None, "tp", None),
            P(None, "tp", None),
            P(None, None, "tp"),
            P(None, None, "tp"),
            P(None, "tp"),
            P(None, "tp"),
            P(("gr", "sp"), "tp", None),
            P("tp", None, None),
        ),
        out_specs=(
            P(None, ("gr", "sp"), "tp", None, None),
            P(None, ("gr", "sp"), "tp", None),
            P(None, ("gr", "sp"), "tp"),
            P(("gr", "sp"), "tp"),
        ),
        check_vma=False,
    )
```

```python
import functools

import jax
import jax.numpy as jnp
from jax import lax
from jax.experimental import pallas as pl
from jax.experimental.pallas import tpu as pltpu
from jax.sharding import PartitionSpec as P

MESH = pl.DeviceIdType.MESH
F32 = jnp.float32
BF16 = jnp.bfloat16
HIGHEST = lax.Precision.HIGHEST


def nt(a, b):
    return lax.dot_general(a, b, (((1,), (1,)), ((), ())), preferred_element_type=F32)


def tn(a, b):
    return lax.dot_general(a, b, (((0,), (0,)), ((), ())), preferred_element_type=F32)


def iota(shape, axis):
    return lax.broadcasted_iota(jnp.int32, shape, axis)


EDGE_TURNS = (0, 2, 1, 3)
RAW_TO_END, RAW_TO_MIDDLE = (2, 3), (2,)
LINE_TO_END, LINE_TO_MIDDLE = (0, 1), (0, 1, 3)
GROUPS = ((0, 1), (2, 3), (4,), (5,))
FIRST = (
    ("gates", 0),
    ("gates", 1),
    ("barrier", 0),
    ("loaded", 0),
    ("edge", 0),
    ("edge", 1),
    ("inner", 0),
    ("gates", 2),
    ("gates", 3),
    ("send", 0),
    ("weights", 0),
    ("line", 0),
    ("same", 0),
    ("other", 0),
    ("own", 0),
)
ORDER = (
    ("own", 0),
    ("own", 1),
    ("queries", 0),
    ("own", 2),
    ("own", 3),
    ("pass", 0),
    ("own", 4),
    ("pass", 1),
    ("own", 5),
    ("pass", 2),
    ("gates", 0),
    ("pass", 3),
    ("widen", 0),
    ("widen", 1),
    ("widen", 2),
    ("pass", 4),
    ("widen", 3),
    ("collect", 0),
    ("pass", 5),
    ("collect", 1),
    ("collect", 2),
    ("collect", 3),
    ("near", 0),
)


def kernel(
    n, tpn,
    prompt, wk_hbm, wv_hbm, wo_hbm, ig_hbm, fg_hbm, ib_hbm, fb_hbm, q_hbm,
    membuf, norm_out, stab_out, read_out,
    xall, wkv, wo, gate_w, biases, query,
    wg, kvs, kvn, kvf, gsend, grecv, xfar, cols, wb, qb, acc, num, nrm, parts, got,
    lsem, frecv, xrecv, drecv, recv, sent,
):
    sp = lax.axis_index("sp")
    tp = lax.axis_index("tp")
    half = n // 2
    cores = 2
    chips = tpn // cores
    seqs, _, block, depth = xfar.shape
    rows = seqs * block
    width = wo.shape[0]
    line = half // 2
    side = sp // half
    local = sp - side * half
    deck, y = local // line, lax.rem(local, line)
    edge = deck == side
    near_base = side * half
    far_base = half - near_base
    x, c = tp // cores, lax.rem(tp, cores)
    partner = x * cores + 1 - c

    barrier = pltpu.get_barrier_semaphore()
    for i in range(half):
        pl.semaphore_signal(
            barrier,
            inc=1,
            device_id={"sp": far_base + lax.rem(local + half // 2 + i, half)},
            device_id_type=MESH,
        )
    for k in range(1, half):
        pl.semaphore_signal(
            barrier,
            inc=1,
            device_id={"sp": near_base + lax.rem(local + k, half)},
            device_id_type=MESH,
        )
    for j in range(1, tpn):
        pl.semaphore_signal(
            barrier, inc=1, device_id={"tp": lax.rem(tp + j, tpn)}, device_id_type=MESH
        )

    first = len(EDGE_TURNS)
    steps, shared = first + len(RAW_TO_END), first + len(RAW_TO_MIDDLE)

    def far_from(k):
        deck_of = 1 - side if k < first else side
        turn = (EDGE_TURNS + RAW_TO_END)[k]
        return deck_of * line + lax.rem(y + line - turn, line)

    def far_to(near_middle, turn):
        deck_of = side if near_middle else 1 - side
        return far_base + deck_of * line + lax.rem(y + turn, line)

    raw_to = [(False, turn) for turn in RAW_TO_END] + [(True, turn) for turn in RAW_TO_MIDDLE]
    line_to = [(False, turn) for turn in LINE_TO_END] + [(True, turn) for turn in LINE_TO_MIDDLE]

    def near_to(deck_of, turn):
        return deck_of * line + lax.rem(y + turn, line)

    pieces = 4

    def load(i):
        base = (near_base if i < pieces // 2 else far_base) + i % (pieces // 2) * (2 * half // pieces)
        part = pl.ds(base * seqs, 2 * half // pieces * seqs)
        return pltpu.make_async_copy(prompt.at[part], xall.at[part], lsem.at[i])

    gate_loads = [
        pltpu.make_async_copy(ig_hbm, gate_w.at[0], lsem.at[4]),
        pltpu.make_async_copy(fg_hbm, gate_w.at[1], lsem.at[4]),
    ]
    weight_loads = [
        pltpu.make_async_copy(wk_hbm, wkv.at[:, :width], lsem.at[5]),
        pltpu.make_async_copy(wv_hbm, wkv.at[:, width:], lsem.at[5]),
    ]
    late_loads = [
        pltpu.make_async_copy(ib_hbm, biases.at[0], lsem.at[6]),
        pltpu.make_async_copy(fb_hbm, biases.at[1], lsem.at[6]),
        pltpu.make_async_copy(q_hbm, query, lsem.at[7]),
        pltpu.make_async_copy(wo_hbm, wo, lsem.at[8]),
    ]

    def arrived(ref, sem):
        pltpu.make_async_copy(ref, ref, sem).wait()

    def send_far(near_middle, turn, slot):
        dest = far_to(near_middle, turn)
        return pltpu.make_async_remote_copy(
            src_ref=xall.at[dest * seqs + tp],
            dst_ref=xfar.at[tp, local],
            send_sem=sent.at[0],
            recv_sem=frecv.at[slot],
            device_id={"sp": dest},
            device_id_type=MESH,
        )

    def far_from_edge(at):
        for slot, turn in enumerate(EDGE_TURNS):
            send_far(at == 1, turn, slot).start()

    def far_from_inner():
        for i, (near_middle, turn) in enumerate(raw_to):
            send_far(near_middle, turn, first + i % len(RAW_TO_END)).start()

    def send_near(deck_of, turn):
        dest = near_to(deck_of, turn)
        return pltpu.make_async_remote_copy(
            src_ref=kvs.at[dest],
            dst_ref=kvn.at[local],
            send_sem=sent.at[1],
            recv_sem=recv.at[0],
            device_id={"sp": near_base + dest},
            device_id_type=MESH,
        )

    def send_line(i):
        return pltpu.make_async_remote_copy(
            src_ref=kvs.at[half + i],
            dst_ref=kvf.at[local],
            send_sem=sent.at[6],
            recv_sem=recv.at[3],
            device_id={"sp": far_to(*line_to[i])},
            device_id_type=MESH,
        )

    def send_gates(k):
        dest = lax.rem(sp + k, n)
        return pltpu.make_async_remote_copy(
            src_ref=gsend.at[dest],
            dst_ref=grecv.at[sp],
            send_sem=sent.at[2],
            recv_sem=recv.at[1],
            device_id={"sp": dest},
            device_id_type=MESH,
        )

    def spread(j, k):
        piece = xfar.at[tp, far_from(k)]
        return pltpu.make_async_remote_copy(
            src_ref=piece,
            dst_ref=piece,
            send_sem=sent.at[3],
            recv_sem=xrecv.at[k],
            device_id={"tp": lax.rem(x + j, chips) * cores + c},
            device_id_type=MESH,
        )

    def group_of(k):
        return [p for p, group in enumerate(GROUPS) if k in group][0]

    def hand(j, k):
        origin = lax.rem(x + chips - j, chips) * cores + c
        piece = xfar.at[origin, far_from(k)]
        return pltpu.make_async_remote_copy(
            src_ref=piece,
            dst_ref=piece,
            send_sem=sent.at[4],
            recv_sem=drecv.at[group_of(k)],
            device_id={"tp": partner},
            device_id_type=MESH,
        )

    def give(j):
        peer = lax.rem(tp + j, tpn)
        return pltpu.make_async_remote_copy(
            src_ref=parts.at[peer],
            dst_ref=got.at[j],
            send_sem=sent.at[5],
            recv_sem=recv.at[2],
            device_id={"tp": peer},
            device_id_type=MESH,
        )

    for copy in gate_loads:
        copy.start()
    for i in range(pieces):
        load(i).start()
    for copy in weight_loads + late_loads:
        copy.start()

    arrived(gate_w, lsem.at[4])
    wg[...] = jnp.concatenate(
        [gate_w[0].astype(F32), gate_w[1].astype(F32), jnp.zeros((wg.shape[0] - 4, depth), F32)],
        axis=0,
    ).astype(BF16)

    def rows_of(dest):
        return xall[pl.ds(dest * seqs, seqs)].reshape(rows, depth)

    def gates(start, stop):
        for i in range(start, stop):
            if i < half and i % (2 * half // pieces) == 0:
                load(i // (2 * half // pieces)).wait()
            dest = (near_base if i < half else far_base) + i % half
            gsend[pl.ds(dest, 1)] = nt(wg[...], rows_of(dest))[:4][None]

    inner = jnp.logical_not(edge)

    def start_gates():
        grecv[pl.ds(sp, 1)] = gsend[pl.ds(sp, 1)]
        for k in range(1, n):
            send_gates(k).start()

    def keys_values(blocks, base):
        lines = [rows_of(dest) for dest in blocks]
        both = jnp.dot(
            jnp.concatenate(lines, axis=0), wkv[...], preferred_element_type=F32
        ).astype(BF16)
        kvs[pl.ds(base, len(blocks))] = both.reshape(len(blocks), rows, 2 * width)

    def near_other():
        base = (1 - deck) * line
        keys_values([near_base + base + i for i in range(line)], base)
        for turn in (0, 2, 1, 3):
            send_near(1 - deck, turn).start()

    def near_same():
        base = deck * line
        keys_values([near_base + base + i for i in range(line)], base)
        for turn in (2, 1, 3):
            send_near(deck, turn).start()

    def own_near():
        kvn[pl.ds(local, 1)] = kvs[pl.ds(local, 1)]

    def lines():
        count = len(line_to)
        keys_values([far_to(*to) for to in line_to], half)
        for i in range(count):
            send_line(i).start()

    first_jobs = {
        "barrier": lambda _: pl.semaphore_wait(barrier, n - 1 + tpn - 1),
        "loaded": lambda _: [load(i).wait() for i in range(pieces // 2, pieces)],
        "edge": lambda at: pl.when(edge)(functools.partial(far_from_edge, at)),
        "inner": lambda _: pl.when(inner)(far_from_inner),
        "gates": lambda at: gates(at * half // 2, (at + 1) * half // 2),
        "send": lambda _: start_gates(),
        "weights": lambda _: arrived(wkv, lsem.at[5]),
        "other": lambda _: near_other(),
        "same": lambda _: near_same(),
        "own": lambda _: own_near(),
        "line": lambda _: pl.when(inner)(lines),
    }
    for job, at in FIRST:
        first_jobs[job](at)

    def weigh():
        lane = iota((rows, rows), 1)
        down = iota((rows, rows), 0)
        same = (lane // block) == (down // block)
        upto = (same & (down <= lane)).astype(F32)
        whole = same.astype(F32)
        before = (
            (iota((2 * n, 2 * n), 0) // n == iota((2 * n, 2 * n), 1) // n)
            & (iota((2 * n, 2 * n), 1) < iota((2 * n, 2 * n), 0))
        ).astype(F32)
        pre = [
            grecv[:, i, :] + biases[i // 2, 0:1, i % 2 : i % 2 + 1]
            for i in range(4)
        ]
        forget_pre = jnp.concatenate(pre[2:], axis=0)
        forget = jnp.minimum(forget_pre, 0.0) - jnp.log1p(jnp.exp(-jnp.abs(forget_pre)))
        inside = jnp.dot(forget, upto, preferred_element_type=F32, precision=HIGHEST)
        sums = jnp.dot(forget, whole, preferred_element_type=F32, precision=HIGHEST)
        running = jnp.dot(before, sums, preferred_element_type=F32, precision=HIGHEST) + inside
        totals = [jnp.sum(sums[g * n : (g + 1) * n], axis=0, keepdims=True) for g in range(2)]
        logs = [
            pre[0] + totals[0] - running[:n],
            pre[1] + running[n:] - forget[n:],
        ]
        peak = jnp.concatenate(
            [jnp.maximum(totals[g], jnp.max(logs[g], axis=0, keepdims=True)) for g in range(2)]
            + [jnp.zeros((6, rows), F32)],
            axis=0,
        )
        spot = iota(peak.shape, 1)
        step = 1
        while step < block:
            low, high = pltpu.roll(peak, step, 1), pltpu.roll(peak, rows - step, 1)
            peak = jnp.maximum(peak, jnp.where((spot & step) != 0, low, high))
            step *= 2
        weight = [jnp.exp(logs[g] - peak[g : g + 1]) * width ** (-0.5) for g in range(2)]
        first = side == 0
        parted = [jnp.where(first, w[:half], w[half:]) for w in weight]
        parted += [jnp.where(first, w[half:], w[:half]) for w in weight]
        cols[...] = jnp.concatenate(parted, axis=0).T
        own = iota((seqs, rows), 1) // block == iota((seqs, rows), 0)
        return [
            jnp.max(jnp.where(own, peak[g : g + 1], -jnp.inf), axis=1, keepdims=True)
            for g in range(2)
        ]

    def widen(i):
        for q in range(seqs):
            for s in range(half):
                j = i * half + s
                wb[i, q, s] = jnp.broadcast_to(
                    cols[q * block : (q + 1) * block, j : j + 1], (block, width)
                )

    def outer(kv, i, q):
        lines = slice(q * block, (q + 1) * block)
        keys = kv[:, lines, :width].reshape(half * block, width)
        values = kv[:, lines, width:].reshape(half * block, width).astype(F32)
        w0 = wb[2 * i, q].reshape(half * block, width)
        w1 = wb[2 * i + 1, q].reshape(half * block, width)
        weighted = jnp.concatenate([values * w0, values * w1], axis=1).astype(BF16)
        keys_f = keys.astype(F32)
        sums = [jnp.sum(keys_f * w, axis=0, keepdims=True) for w in (w0, w1)]
        return tn(keys, weighted), sums

    def project(p):
        found = [far_from(k) for k in GROUPS[p]]
        lines = [xfar[:, pl.ds(source, 1)].reshape(rows, depth) for source in found]
        both = jnp.dot(
            jnp.concatenate(lines, axis=0), wkv[...], preferred_element_type=F32
        ).astype(BF16)
        for i, source in enumerate(found):
            kvf[pl.ds(source, 1)] = both[i * rows : (i + 1) * rows][None]

    def own(k):
        arrived(xfar.at[0, 0], frecv.at[k])
        for j in (2, 1, 3):
            spread(j, k).start()
        hand(0, k).start()

    def pass_on(k):
        arrived(xfar.at[pl.ds(1, chips - 1), 0], xrecv.at[k])
        for j in (1, 3, 2):
            hand(j, k).start()

    def collect(p):
        arrived(xfar.at[pl.ds(0, chips), pl.ds(0, len(GROUPS[p]))], drecv.at[p])
        project(p)

    def queries():
        arrived(biases, lsem.at[6])
        for copy in late_loads[2:]:
            copy.wait()
        turned = query[...].astype(F32).T
        for q in range(seqs):
            qb[q] = jnp.broadcast_to(turned[:, q : q + 1], (width, width))

    stables = []

    def gates_in():
        arrived(grecv.at[pl.ds(0, n - 1)], recv.at[1])
        stables.extend(weigh())

    def widened(i):
        widen(i)

    def near_part():
        arrived(kvn.at[pl.ds(0, half - 1)], recv.at[0])
        for q in range(seqs):
            acc[q], sums = outer(kvn, 0, q)
            for g in range(2):
                nrm[g, q : q + 1] = sums[g]

    jobs = {
        "own": own, "pass": pass_on, "collect": collect, "widen": widened,
        "queries": lambda _: queries(), "gates": lambda _: gates_in(), "near": lambda _: near_part(),
    }
    for job, at in ORDER:
        slot = GROUPS[at][0] if job == "collect" else at if job in ("own", "pass") else 0
        if slot < shared:
            jobs[job](at)
        else:
            pl.when(edge)(functools.partial(jobs[job], at))
    @pl.when(edge)
    def _():
        arrived(kvf.at[pl.ds(0, len(LINE_TO_END))], recv.at[3])

    @pl.when(inner)
    def _():
        arrived(kvf.at[pl.ds(0, len(LINE_TO_MIDDLE))], recv.at[3])

    for q in range(seqs):
        more, sums = outer(kvf, 1, q)
        memory = (acc[q] + more).astype(BF16)
        back = memory.astype(F32)
        for g in range(2):
            membuf[g, q, 0] = memory[:, g * width : (g + 1) * width]
            num[g, q : q + 1] = jnp.sum(
                qb[q] * back[:, g * width : (g + 1) * width], axis=0, keepdims=True
            )
            total = nrm[g, q : q + 1] + sums[g]
            nrm[g, q : q + 1] = total
            norm_out[g, q] = total

    hidden = jnp.zeros((seqs, width), F32)
    queries = query[...].astype(F32)
    for g in range(2):
        under = jnp.abs(jnp.sum(queries * nrm[g], axis=1, keepdims=True))
        floor = jnp.maximum(jnp.exp(-stables[g]), 1.0)
        hidden = hidden + num[g] / jnp.maximum(under, floor)
        square = iota((seqs, width), 1) == iota((seqs, width), 0)
        row = jnp.sum(jnp.where(square, stables[g], 0.0), axis=0, keepdims=True)
        stab_out[g] = row[:, :seqs]
    terms = jnp.dot(hidden.astype(BF16), wo[...], preferred_element_type=F32)
    share = terms.shape[1] // tpn
    for t in range(tpn):
        parts[t] = terms[:, t * share : (t + 1) * share]
    for j in sorted(range(1, tpn), key=lambda j: abs(j - tpn / 2)):
        give(j).start()
    def passed(count):
        arrived(xfar.at[pl.ds(0, chips - 1), pl.ds(0, count)], sent.at[3])
        arrived(xfar.at[pl.ds(0, chips), pl.ds(0, count)], sent.at[4])

    @pl.when(edge)
    def _():
        arrived(xfar.at[0, pl.ds(0, 2 * first)], sent.at[0])
        passed(steps)

    @pl.when(inner)
    def _():
        arrived(xfar.at[0, pl.ds(0, len(raw_to))], sent.at[0])
        arrived(kvs.at[pl.ds(0, len(line_to))], sent.at[6])
        passed(shared)

    arrived(kvs.at[pl.ds(0, half - 1)], sent.at[1])
    arrived(grecv.at[pl.ds(0, n - 1)], sent.at[2])
    arrived(got.at[pl.ds(0, tpn - 1)], sent.at[5])
    arrived(got.at[pl.ds(0, tpn - 1)], recv.at[2])
    total = parts[tp]
    for j in range(1, tpn):
        total = total + got[j]
    read_out[...] = total.astype(BF16)


def publish(count, *refs):
    sources, targets, sems = refs[:count], refs[count : 2 * count], refs[2 * count]
    copies = [
        pltpu.make_async_copy(a, b, sems.at[i]) for i, (a, b) in enumerate(zip(sources, targets))
    ]
    for copy in copies:
        copy.start()
    for copy in copies:
        copy.wait()


def solution(mesh):
    n, tpn = mesh.shape["sp"], mesh.shape["tp"]

    def body(prompt, w_key, w_value, w_in_gate, w_forget_gate, in_bias, forget_bias, query, w_out):
        depth, heads, width = w_key.shape
        seqs = prompt.shape[0] // n
        block = prompt.shape[1]
        rows = seqs * block
        half = n // 2
        chips = tpn // 2
        steps = len(EDGE_TURNS) + len(RAW_TO_END)
        wo = w_out.reshape(heads * width, -1)
        columns = wo.shape[1]
        any_ = pl.BlockSpec(memory_space=pl.ANY)
        vmem = pl.BlockSpec(memory_space=pltpu.VMEM)
        dma = pltpu.SemaphoreType.DMA
        shapes = (
            ((2, seqs, heads, width, width), BF16),
            ((2, seqs, heads, width), F32),
            ((2, heads, seqs), F32),
            ((seqs, columns // tpn), BF16),
        )
        held = pl.pallas_call(
            functools.partial(kernel, n, tpn),
            out_shape=tuple(pltpu.VMEM(*shape) for shape in shapes),
            in_specs=[any_] * 9,
            out_specs=(vmem,) * 4,
            scratch_shapes=[
                pltpu.VMEM((n * seqs, block, depth), BF16),
                pltpu.VMEM((depth, 2 * width), BF16),
                pltpu.VMEM((width, columns), BF16),
                pltpu.VMEM((2, 2, depth), BF16),
                pltpu.VMEM((2, 1, 2), F32),
                pltpu.VMEM((seqs, width), BF16),
                pltpu.VMEM((16, depth), BF16),
                pltpu.VMEM((half + len(LINE_TO_END + LINE_TO_MIDDLE), rows, 2 * width), BF16),
                pltpu.VMEM((half, rows, 2 * width), BF16),
                pltpu.VMEM((half, rows, 2 * width), BF16),
                pltpu.VMEM((n, 4, rows), F32),
                pltpu.VMEM((n, 4, rows), F32),
                pltpu.VMEM((seqs, half, block, depth), BF16),
                pltpu.VMEM((rows, 4 * half), F32),
                pltpu.VMEM((4, seqs, half, block, width), F32),
                pltpu.VMEM((seqs, width, width), F32),
                pltpu.VMEM((seqs, width, 2 * width), F32),
                pltpu.VMEM((2, seqs, width), F32),
                pltpu.VMEM((2, seqs, width), F32),
                pltpu.VMEM((tpn, seqs, columns // tpn), F32),
                pltpu.VMEM((tpn, seqs, columns // tpn), F32),
                dma((9,)),
                dma((steps,)),
                dma((steps,)),
                dma((len(GROUPS),)),
                dma((4,)),
                dma((7,)),
            ],
            compiler_params=pltpu.CompilerParams(collective_id=0, has_side_effects=True),
            name="memories",
        )(
            prompt, w_key.reshape(depth, width), w_value.reshape(depth, width), wo,
            w_in_gate.reshape(2, depth), w_forget_gate.reshape(2, depth),
            in_bias.reshape(1, 2), forget_bias.reshape(1, 2), query.reshape(seqs, width),
        )
        memory, normal, stable, read = pl.pallas_call(
            functools.partial(publish, len(shapes)),
            out_shape=tuple(jax.ShapeDtypeStruct(*shape) for shape in shapes),
            in_specs=[vmem] * len(shapes),
            out_specs=(any_,) * len(shapes),
            scratch_shapes=[dma((len(shapes),))],
            name="outputs",
        )(*[pltpu.with_memory_space_constraint(a, pltpu.VMEM) for a in held])
        return memory, normal, stable.transpose(0, 2, 1), read

    return jax.shard_map(
        body,
        mesh=mesh,
        in_specs=(
            P("gr", "sp", None),
            P(None, "tp", None),
            P(None, "tp", None),
            P(None, None, "tp"),
            P(None, None, "tp"),
            P(None, "tp"),
            P(None, "tp"),
            P(("gr", "sp"), "tp", None),
            P("tp", None, None),
        ),
        out_specs=(
            P(None, ("gr", "sp"), "tp", None, None),
            P(None, ("gr", "sp"), "tp", None),
            P(None, ("gr", "sp"), "tp"),
            P(("gr", "sp"), "tp"),
        ),
        check_vma=False,
    )
```
